32 devices in a mesh: sp: 4 (over x, core), tp: 8 (over z, y).
Axes of the slice: x: 2, y: 2, z: 4, core: 2. Of those that a mesh axis runs over, the one named last changes fastest.
Arguments:
- latent: bfloat16 [512, 4096], P('sp', 'tp'), may hold values from -60 to 60
- context: bfloat16 [64, 4096], P('sp', 'tp'), may hold values from -6 to 6
- conditioning: bfloat16 [4096], P('sp'), may hold values from -6 to 6
- context_prompt_vector: bfloat16 [4096], P('sp'), may hold values from -6 to 6
- shift_matrix: bfloat16 [4096, 4096], P('tp', 'sp'), may hold values from -0.09375 to 0.09375
- scale_matrix: bfloat16 [4096, 4096], P('tp', 'sp'), may hold values from -0.09375 to 0.09375
- residual_gate_matrix: bfloat16 [4096, 4096], P('tp', 'sp'), may hold values from -0.09375 to 0.09375
- query_matrix: bfloat16 [2048, 4096], P('tp'), may hold values from -0.09375 to 0.09375
- key_matrix: bfloat16 [2048, 4096], P('tp'), may hold values from -0.09375 to 0.09375
- value_matrix: bfloat16 [4096, 4096], P('tp'), may hold values from -0.09375 to 0.09375
- gate_matrix: bfloat16 [4096, 4096], P('tp'), may hold values from -0.09375 to 0.09375
- decay_down_factor: bfloat16 [2, 4096, 16], replicated, may hold values from -0.09375 to 0.09375
- decay_up_factor: bfloat16 [2, 16, 2048], replicated, may hold values from -1.5 to 1.5
- decay_key_bias: float32 [2, 2048], replicated, may hold values from -0.5 to 7
- spike_log_decay: float32 [2, 512, 16], P(None, 'sp'), may hold values from -2.8 to 0
- output_gain: float32 [4096], P('tp'), may hold values from 0.1 to 1.9
- output_matrix: bfloat16 [4096, 4096], P('tp'), may hold values from -0.375 to 0.375
Outputs:
- mixed: bfloat16 [512, 4096], P('sp', 'tp')
The draws below stay inside these ranges and needn't reach their ends.
All inputs are finite; a program needn't handle non-finite values.
Results may differ from the reference program's by a relative error of at most 0.013.
Values may be sent and summed in bfloat16 or wider, within the bound.
A program may use at most 64 MiB of HBM per device.

```python
import math
import jax
import jax.numpy as jnp
from jax import lax

D = 4096
HEADS = 16
DK = 128
DV = 256
DECAY_RANK = 16
BLK = 64
VGROUP = 64
SEQ = 512
CTX = 64


def draw_latent(key, part):
    key_one, key_two = jax.random.split(key, 2)
    normal_part = jnp.clip(jax.random.normal(key_one, (SEQ, D), jnp.float32), -5.0, 5.0)
    column_rise = jnp.exp(jnp.linspace(math.log(0.6), math.log(2.0), D))
    jitter = jax.random.uniform(key_two, (1, D), jnp.float32, 0.7, 1.4)
    return (normal_part * column_rise * jitter).astype(jnp.bfloat16)


def draw_decay_key_bias(key, part):
    key_one, key_two, key_three = jax.random.split(key, 3)
    fast_share = 0.5
    fast_heads = jax.random.bernoulli(key_one, fast_share, (2, HEADS, 1))
    fast_rates = jax.random.uniform(key_two, (2, HEADS, DK), jnp.float32, -0.5, 1.5)
    slow_rates = jax.random.uniform(key_three, (2, HEADS, DK), jnp.float32, 5.0, 7.0)
    return jnp.where(fast_heads, fast_rates, slow_rates).reshape(2, HEADS * DK)


def draw_spike_log_decay(key, part):
    key_one, key_two = jax.random.split(key, 2)
    spots = jax.random.randint(key_one, (2, HEADS, 4), 0, SEQ)
    depths = jnp.log(jax.random.uniform(key_two, (2, HEADS, 4), jnp.float32, 0.5, 0.8))
    positions = jnp.arange(SEQ, dtype=jnp.int32)
    hits = (positions[None, None, None, :] == spots[:, :, :, None]).astype(jnp.float32)
    summed = jnp.sum(hits * depths[:, :, :, None], axis=2)
    return jnp.transpose(summed, (0, 2, 1))


def level_of(rng, dims, cuts, least, top_value):
    factor_of, own = 1.0, jax.random.fold_in(rng, 6)
    for position, blocks in cuts:
        heights = jnp.exp(jax.random.uniform(jax.random.fold_in(own, position), (blocks,), jnp.float32, least / len(cuts), top_value / len(cuts)))
        factor_of = factor_of * jnp.repeat(heights, dims[position] // blocks).reshape([-1 if axis == position else 1 for axis in range(len(dims))])
    return factor_of


def centred(own_key, shape, deviation, reach, shards=(), held_as=jnp.bfloat16):
    entries = jax.random.normal(own_key, shape, jnp.float32) * deviation
    if len(shards) > 0:
        entries = level_of(own_key, shape, shards, -0.22, 0.18) * entries
    return jnp.clip(entries, min=-reach, max=reach).astype(held_as)


def setup_inputs(seed: int = 0) -> dict:
    splits = jax.random.split(jax.random.key(seed), 18)
    latent = draw_latent(jax.random.fold_in(splits[17], 71), 0)
    context = centred(splits[1], (CTX, D), 1.0, 6.0, ((0, 4), (1, 8)))
    conditioning = centred(splits[2], (D,), 1.0, 6.0, ((0, 4),))
    context_prompt_vector = centred(splits[3], (D,), 1.0, 6.0, ((0, 4),))
    shift_matrix = centred(splits[4], (D, D), D ** -0.5, 0.09375, ((0, 8), (1, 4)))
    scale_matrix = centred(splits[5], (D, D), D ** -0.5, 0.09375, ((0, 8), (1, 4)))
    residual_gate_matrix = centred(splits[6], (D, D), D ** -0.5, 0.09375, ((0, 8), (1, 4)))
    query_matrix = centred(splits[7], (HEADS * DK, D), D ** -0.5, 0.09375, ((0, 8),))
    key_matrix = centred(splits[8], (HEADS * DK, D), D ** -0.5, 0.09375, ((0, 8),))
    value_matrix = centred(splits[9], (HEADS * DV, D), D ** -0.5, 0.09375, ((0, 8),))
    gate_matrix = centred(splits[10], (HEADS * DV, D), D ** -0.5, 0.09375, ((0, 8),))
    decay_down_factor = centred(splits[11], (2, D, DECAY_RANK), D ** -0.5, 0.09375)
    decay_up_factor = centred(splits[12], (2, DECAY_RANK, HEADS * DK), DECAY_RANK ** -0.5, 1.5)
    decay_key_bias = draw_decay_key_bias(jax.random.fold_in(splits[17], 71), 0)
    spike_log_decay = draw_spike_log_decay(jax.random.fold_in(splits[17], 71), 0)
    output_gain = jnp.clip(1.0 + 0.18 * jax.random.normal(splits[15], (HEADS * DV,), jnp.float32), 0.1, 1.9)
    output_matrix = centred(splits[16], (D, HEADS * DV), (HEADS * DV // 16) ** -0.5, 0.375, ((0, 8),))
    return {"latent": latent, "context": context, "conditioning": conditioning, "context_prompt_vector": context_prompt_vector, "shift_matrix": shift_matrix, "scale_matrix": scale_matrix, "residual_gate_matrix": residual_gate_matrix, "query_matrix": query_matrix, "key_matrix": key_matrix, "value_matrix": value_matrix, "gate_matrix": gate_matrix, "decay_down_factor": decay_down_factor, "decay_up_factor": decay_up_factor, "decay_key_bias": decay_key_bias, "spike_log_decay": spike_log_decay, "output_gain": output_gain, "output_matrix": output_matrix}


epsilon = 1e-05
gate_norm = 16.0
precise = lax.Precision.HIGHEST

def linear(rows, weight):
    return lax.dot_general(rows, weight, (((1,), (1,)), ((), ())), preferred_element_type=jnp.float32)

def modulated(rows, shift_vec, scale_vec):
    rows_f = rows.astype(jnp.float32)
    mean_val = lax.optimization_barrier(jnp.mean(rows_f, axis=-1, keepdims=True))
    variance = lax.optimization_barrier(jnp.mean(rows_f * rows_f, axis=-1, keepdims=True)) - mean_val * mean_val
    return ((rows_f - mean_val) * lax.rsqrt(variance + epsilon) * (1.0 + scale_vec) + shift_vec).astype(jnp.bfloat16)

def reverse_rows(array):
    return jnp.flip(array, axis=0)

def end_state(key_rows, value_rows, log_decay):
    cumulative = jnp.cumsum(log_decay, axis=0)
    totals = cumulative[-1]
    weighted = key_rows * jnp.exp(totals - cumulative)
    return (jnp.exp(totals), jnp.einsum('nhd,nhe->hde', weighted, value_rows, precision=precise))

def blockwise(queries, key_rows, value_rows, log_decay, carried, block_len):
    length, head_count, _ = queries.shape
    value_width = value_rows.shape[-1]
    blocks = length // block_len

    def shaped(array):
        return array.reshape(blocks, block_len, head_count, array.shape[-1])
    triangle = jnp.tril(jnp.ones((block_len, block_len), jnp.float32))

    def advance(state_now, inputs):
        block_q, block_k, block_v, block_a = inputs
        cumulative = jnp.cumsum(block_a, axis=0)
        block_end = cumulative[-1]
        query_dec = block_q * jnp.exp(cumulative)
        scores = jnp.einsum('ihd,jhd->hij', query_dec, block_k * jnp.exp(-cumulative), precision=precise) * triangle
        result = jnp.einsum('hij,jhe->ihe', scores, block_v, precision=precise)
        result = result + jnp.einsum('ihd,hde->ihe', query_dec, state_now, precision=precise)
        state_next = state_now * jnp.exp(block_end)[:, :, None] + jnp.einsum('jhd,jhe->hde', block_k * jnp.exp(block_end - cumulative), block_v, precision=precise)
        return (state_next, result)
    _, outputs = lax.scan(advance, carried, (shaped(queries), shaped(key_rows), shaped(value_rows), shaped(log_decay)))
    return outputs.reshape(length, head_count, value_width)

def reference(latent, context, conditioning, context_prompt_vector, shift_matrix, scale_matrix, residual_gate_matrix, query_matrix, key_matrix, value_matrix, gate_matrix, decay_down_factor, decay_up_factor, decay_key_bias, spike_log_decay, output_gain, output_matrix):
    conds = jax.nn.silu(jnp.stack([conditioning, context_prompt_vector]).astype(jnp.float32)).astype(jnp.bfloat16)
    shifts = linear(conds, shift_matrix)
    scales = linear(conds, scale_matrix)
    gates = linear(conds, residual_gate_matrix)
    latent_normalized = modulated(latent, shifts[0], scales[0])
    normed_ctx = modulated(context, shifts[1], scales[1])

    def project(rows, weight):
        stored = lax.optimization_barrier(linear(rows, weight).astype(jnp.bfloat16))
        return stored.astype(jnp.float32)

    def split_heads(rows, width):
        return rows.reshape(rows.shape[0], HEADS, width)
    queries = split_heads(project(latent_normalized, query_matrix), DK) * DK ** (-0.5)
    key_rows = split_heads(project(latent_normalized, key_matrix), DK)
    value_rows = split_heads(project(latent_normalized, value_matrix), DV)
    gate_rows = project(latent_normalized, gate_matrix)
    ctx_keys = split_heads(project(normed_ctx, key_matrix), DK)
    ctx_values = split_heads(project(normed_ctx, value_matrix), DV)

    def per_head_decay(rows, direction):
        low_rows = jnp.dot(rows, decay_down_factor[direction], preferred_element_type=jnp.float32)
        pre_act = jnp.dot(low_rows, decay_up_factor[direction].astype(jnp.float32), precision=precise) + decay_key_bias[direction]
        return split_heads(jax.nn.log_sigmoid(pre_act) / gate_norm, DK)
    latent_forward = per_head_decay(latent_normalized, 0) + spike_log_decay[0][:, :, None]
    latent_backward = per_head_decay(latent_normalized, 1) + spike_log_decay[1][:, :, None]
    ctx_fwd = per_head_decay(normed_ctx, 0)
    ctx_bwd = per_head_decay(normed_ctx, 1)
    start_fwd = end_state(ctx_keys, ctx_values, ctx_fwd)[1]
    start_bwd = end_state(reverse_rows(ctx_keys), reverse_rows(ctx_values), reverse_rows(ctx_bwd))[1]
    out_fwd = blockwise(queries, key_rows, value_rows, latent_forward, start_fwd, BLK)
    out_bwd = reverse_rows(blockwise(reverse_rows(queries), reverse_rows(key_rows), reverse_rows(value_rows), reverse_rows(latent_backward), start_bwd, BLK))
    grouped = (out_fwd + out_bwd).reshape(SEQ, HEADS * DV // VGROUP, VGROUP)
    grouped = grouped * lax.rsqrt(lax.optimization_barrier(jnp.mean(grouped * grouped, axis=-1, keepdims=True)) + epsilon)
    heads_out = (grouped.reshape(SEQ, HEADS * DV) * output_gain * jax.nn.silu(gate_rows)).astype(jnp.bfloat16)
    branch = linear(heads_out, output_matrix)
    return (latent.astype(jnp.float32) + gates[0] * branch).astype(jnp.bfloat16)
```

```python
import functools

import jax
import jax.numpy as jnp
from jax import lax
from jax.experimental import pallas as pl
from jax.experimental.pallas import tpu as pltpu
from jax.sharding import PartitionSpec as P

D = 4096
HEADS = 16
DK = 128
DECAY_RANK = 16
BLK = 64
VGROUP = 64
MESH = pl.DeviceIdType.MESH


epsilon = 1e-05
gate_norm = 16.0
precise = lax.Precision.HIGHEST


def for_sending(value):

    def short(part):
        return part.astype(jnp.bfloat16) if part.dtype == jnp.float32 else part

    return jax.tree.map(short, value)


def from_partner(value, axis, distance):
    return lax.ppermute(value, axis, [(i, i ^ 1 << distance) for i in range(lax.axis_size(axis))])


def carried_in(value, axis, combine, identity, reverse):
    peers, index = (lax.axis_size(axis), lax.axis_index(axis))
    everything = jax.tree.map(
        lambda part, kind: lax.all_gather(part.astype(kind), axis),
        value,
        (jnp.bfloat16, jnp.bfloat16),
    )
    start = jax.tree.map(
        lambda part, zero: jnp.broadcast_to(jnp.asarray(zero, part.dtype), part.shape),
        value,
        identity,
    )

    def turn(k, before):
        at = peers - 1 - k if reverse else k
        reached = at > index if reverse else at < index
        new = combine(
            before, jax.tree.map(lambda part, own: part[at].astype(own.dtype), everything, value)
        )
        return jax.tree.map(lambda a, b: jnp.where(reached, a, b), new, before)

    return lax.fori_loop(0, peers, turn, start)


def linear(rows, weight):
    return lax.dot_general(
        rows, weight, (((1,), (1,)), ((), ())), preferred_element_type=jnp.float32
    )


def modulated(rows, row_sum, row_squares, shift_vec, scale_vec):
    rows_f = rows.astype(jnp.float32)
    mean_val = row_sum / D
    variance = row_squares / D - mean_val * mean_val
    return (
        (rows_f - mean_val) * lax.rsqrt(variance + epsilon) * (1.0 + scale_vec) + shift_vec
    ).astype(jnp.bfloat16)


def reverse_rows(array):
    return jnp.flip(array, axis=0)


def end_state(key_rows, value_rows, log_decay):
    cumulative = jnp.cumsum(log_decay, axis=0)
    totals = cumulative[-1]
    weighted = key_rows * jnp.exp(totals - cumulative)
    return (jnp.exp(totals), jnp.einsum("nhd,nhe->hde", weighted, value_rows, precision=precise))


def combine(earlier, later):
    return (earlier[0] * later[0], later[0][..., None] * earlier[1] + later[1])


def blockwise(queries, key_rows, value_rows, log_decay, carried, block_len):
    length, head_count, _ = queries.shape
    value_width = value_rows.shape[-1]
    blocks = length // block_len

    def shaped(array):
        return array.reshape(blocks, block_len, head_count, array.shape[-1])

    triangle = jnp.tril(jnp.ones((block_len, block_len), jnp.float32))

    def advance(state_now, inputs):
        block_q, block_k, block_v, block_a = inputs
        cumulative = jnp.cumsum(block_a, axis=0)
        block_end = cumulative[-1]
        query_dec = block_q * jnp.exp(cumulative)
        scores = (
            jnp.einsum("ihd,jhd->hij", query_dec, block_k * jnp.exp(-cumulative), precision=precise)
            * triangle
        )
        result = jnp.einsum("hij,jhe->ihe", scores, block_v, precision=precise)
        result = result + jnp.einsum("ihd,hde->ihe", query_dec, state_now, precision=precise)
        state_next = state_now * jnp.exp(block_end)[:, :, None] + jnp.einsum(
            "jhd,jhe->hde", block_k * jnp.exp(block_end - cumulative), block_v, precision=precise
        )
        return (state_next, result)

    _, outputs = lax.scan(
        advance, carried, (shaped(queries), shaped(key_rows), shaped(value_rows), shaped(log_decay))
    )
    return outputs.reshape(length, head_count, value_width)


def head_channels(pieces, per_head, tp_index):
    for bit_number in range(per_head.bit_length() - 1):
        partner = from_partner(
            (for_sending(pieces[0]), for_sending(pieces[1]), for_sending(pieces[2])),
            "tp",
            bit_number,
        )
        upper = tp_index // (1 << bit_number) % 2 == 1
        pieces = tuple(
            (
                jnp.where(
                    upper,
                    jnp.concatenate([theirs, mine], axis=1),
                    jnp.concatenate([mine, theirs], axis=1),
                )
                for mine, theirs in zip(pieces, partner)
            )
        )
    return pieces


def context_totals(fwd_growth, fwd_state, bwd_growth, bwd_state, identity):

    def absorb(carried, piece):
        return (combine(carried, piece), None)

    total_fwd, _ = lax.scan(absorb, identity, (fwd_growth, fwd_state))
    total_bwd, _ = lax.scan(absorb, identity, (bwd_growth, bwd_state), reverse=True)
    return (total_fwd, total_bwd)


def stored(array):
    return lax.optimization_barrier(array.astype(jnp.bfloat16))


def local(
    latent,
    context,
    conditioning,
    context_prompt_vector,
    shift_matrix,
    scale_matrix,
    residual_gate_matrix,
    query_matrix,
    key_matrix,
    value_matrix,
    gate_matrix,
    decay_down_factor,
    decay_up_factor,
    decay_key_bias,
    spike_log_decay,
    output_gain,
    output_matrix,
):
    tp_count = lax.axis_size("tp")
    tp_index = lax.axis_index("tp")
    per_head = max(tp_count // HEADS, 1)
    heads_per_shard = max(HEADS // tp_count, 1)
    leading_head = tp_index // per_head * heads_per_shard
    tok_rows = latent.shape[0]
    conds = jax.nn.silu(
        jnp.stack([conditioning, context_prompt_vector]).astype(jnp.float32)
    ).astype(jnp.bfloat16)
    shifts, scales, gates = lax.psum(
        (
            linear(conds, shift_matrix),
            linear(conds, scale_matrix),
            linear(conds, residual_gate_matrix),
        ),
        "sp",
    )
    down_both = jnp.concatenate([decay_down_factor[0].T, decay_down_factor[1].T], axis=0)
    lat_weights = (query_matrix, key_matrix, value_matrix, gate_matrix, down_both)
    ctx_weights = (key_matrix, value_matrix, down_both)
    lat_f = latent.astype(jnp.float32)
    ctx_f = context.astype(jnp.float32)
    lat_sum, lat_squares, ctx_sum, ctx_squares = lax.psum(
        (
            jnp.sum(lat_f, axis=1, keepdims=True),
            jnp.sum(lat_f * lat_f, axis=1, keepdims=True),
            jnp.sum(ctx_f, axis=1, keepdims=True),
            jnp.sum(ctx_f * ctx_f, axis=1, keepdims=True),
        ),
        "tp",
    )
    latent_normalized = modulated(latent, lat_sum, lat_squares, shifts[0], scales[0])
    normed_ctx = modulated(context, ctx_sum, ctx_squares, shifts[1], scales[1])
    lat_piece = lax.all_gather(latent_normalized, "tp", axis=1, tiled=True)
    ctx_piece = lax.all_gather(normed_ctx, "tp", axis=1, tiled=True)
    lat_new = tuple((linear(lat_piece, weight) for weight in lat_weights))
    ctx_new = tuple((linear(ctx_piece, weight) for weight in ctx_weights))
    query_part, key_part, value_part, gate_part, low_rank_part = lat_new
    ctx_key_part, ctx_value_part, ctx_low = ctx_new
    query_full, key_full, ctx_key_full = head_channels(
        (stored(query_part), stored(key_part), stored(ctx_key_part)), per_head, tp_index
    )

    def split_heads(rows, width):
        return rows.astype(jnp.float32).reshape(rows.shape[0], heads_per_shard, width)

    value_cols = value_part.shape[1] // heads_per_shard
    queries = split_heads(query_full, DK) * DK ** (-0.5)
    key_rows = split_heads(key_full, DK)
    ctx_keys = split_heads(ctx_key_full, DK)
    values_lat = split_heads(stored(value_part), value_cols)
    values_ctx = split_heads(stored(ctx_value_part), value_cols)
    gate_rows = stored(gate_part).astype(jnp.float32)

    def per_head_decay(low_rows, direction):
        up_part = lax.dynamic_slice_in_dim(
            decay_up_factor[direction], leading_head * DK, heads_per_shard * DK, 1
        ).astype(jnp.float32)
        bias_part = lax.dynamic_slice_in_dim(
            decay_key_bias[direction], leading_head * DK, heads_per_shard * DK, 0
        )
        pre_act = jnp.dot(low_rows, up_part, precision=precise) + bias_part
        return (jax.nn.log_sigmoid(pre_act) / gate_norm).reshape(
            low_rows.shape[0], heads_per_shard, DK
        )

    decay_spikes = lax.dynamic_slice_in_dim(spike_log_decay, leading_head, heads_per_shard, 2)
    latent_forward = per_head_decay(low_rank_part[:, :DECAY_RANK], 0) + decay_spikes[0][:, :, None]
    latent_backward = per_head_decay(low_rank_part[:, DECAY_RANK:], 1) + decay_spikes[1][:, :, None]
    ctx_fwd = per_head_decay(ctx_low[:, :DECAY_RANK], 0)
    ctx_bwd = per_head_decay(ctx_low[:, DECAY_RANK:], 1)
    cf_growth, cf_state = end_state(ctx_keys, values_ctx, ctx_fwd)
    cb_growth, cb_state = end_state(
        reverse_rows(ctx_keys), reverse_rows(values_ctx), reverse_rows(ctx_bwd)
    )
    lf_growth, lf_state = end_state(key_rows, values_lat, latent_forward)
    lb_growth, lb_state = end_state(
        reverse_rows(key_rows), reverse_rows(values_lat), reverse_rows(latent_backward)
    )
    identity = (
        jnp.ones((heads_per_shard, DK), jnp.float32),
        jnp.zeros((heads_per_shard, DK, value_cols), jnp.float32),
    )
    ctx_gathered = (
        lax.all_gather(cf_growth[None].astype(jnp.bfloat16), "sp", axis=0, tiled=True).astype(
            jnp.float32
        ),
        lax.all_gather(cf_state[None].astype(jnp.bfloat16), "sp", axis=0, tiled=True).astype(
            jnp.float32
        ),
        lax.all_gather(cb_growth[None].astype(jnp.bfloat16), "sp", axis=0, tiled=True).astype(
            jnp.float32
        ),
        lax.all_gather(cb_state[None].astype(jnp.bfloat16), "sp", axis=0, tiled=True).astype(
            jnp.float32
        ),
    )
    total_fwd, total_bwd = context_totals(
        ctx_gathered[0], ctx_gathered[1], ctx_gathered[2], ctx_gathered[3], identity
    )
    prefix = carried_in((lf_growth, lf_state), "sp", combine, identity, False)
    suffix = carried_in((lb_growth, lb_state), "sp", combine, identity, True)
    start_fwd = combine(total_fwd, prefix)[1]
    start_bwd = combine(total_bwd, suffix)[1]
    zero_state = jnp.zeros((heads_per_shard, DK, value_cols), jnp.float32)

    def direction_out(query_rows, key_list, value_list, log_decay, start_state):
        local_part = blockwise(query_rows, key_list, value_list, log_decay, zero_state, BLK)
        reach = query_rows * jnp.exp(jnp.cumsum(log_decay, axis=0))
        return local_part + jnp.einsum("nhd,hde->nhe", reach, start_state, precision=precise)

    out_fwd = direction_out(queries, key_rows, values_lat, latent_forward, start_fwd)
    out_bwd = reverse_rows(
        direction_out(
            reverse_rows(queries),
            reverse_rows(key_rows),
            reverse_rows(values_lat),
            reverse_rows(latent_backward),
            start_bwd,
        )
    )
    grouped = (out_fwd + out_bwd).reshape(tok_rows, -1, VGROUP)
    grouped = grouped * lax.rsqrt(jnp.mean(grouped * grouped, axis=-1, keepdims=True) + epsilon)
    heads_out = (grouped.reshape(tok_rows, -1) * output_gain * jax.nn.silu(gate_rows)).astype(
        jnp.bfloat16
    )
    branch = linear(lax.all_gather(heads_out, "tp", axis=1, tiled=True), output_matrix)
    return (latent.astype(jnp.float32) + gates[0] * branch).astype(jnp.bfloat16)


def exact(a, b):
    return lax.dot_general(
        a, b, (((1,), (0,)), ((), ())), precision=precise, preferred_element_type=jnp.float32
    )


def nt(a, b):
    return lax.dot_general(a, b, (((1,), (1,)), ((), ())), preferred_element_type=jnp.float32)


def nn(a, b):
    return lax.dot_general(a, b, (((1,), (0,)), ((), ())), preferred_element_type=jnp.float32)


def tn(a, b):
    return lax.dot_general(a, b, (((0,), (0,)), ((), ())), preferred_element_type=jnp.float32)


def short(value):
    return value.astype(jnp.bfloat16)


def log_decay_of(low, up, bias):
    pre = exact(low, up) + bias
    return (jnp.minimum(pre, 0.0) - jnp.log1p(jnp.exp(-jnp.abs(pre)))) / gate_norm


def triangle_of(size, upper):
    i = lax.broadcasted_iota(jnp.int32, (size, size), 0)
    j = lax.broadcasted_iota(jnp.int32, (size, size), 1)
    return (j >= i) if upper else (j <= i)


def layer_kernel(
    n,
    s,
    rows,
    crows,
    feats,
    heads,
    dv,
    latent,
    context,
    conditioning,
    prompt,
    shift_m,
    scale_m,
    gate_m,
    query_m,
    key_m,
    value_m,
    og_m,
    down,
    up,
    bias,
    spike,
    gain,
    out_m,
    out_ref,
    x_all,
    xn,
    mod_w,
    proj_w,
    out_w,
    down_v,
    up_v,
    bias_v,
    spike_v,
    gain_v,
    cond_v,
    mod_own,
    mod_recv,
    mod_all,
    proj,
    ctx_kv,
    ctx_low,
    tot_own,
    tot_recv,
    st_own,
    st_recv,
    local_out,
    ho_all,
    load_sem,
    lat_s,
    lat_r,
    ctx_s,
    ctx_r,
    m1_s,
    m1_r,
    m2_s,
    m2_r,
    kv_s,
    kv_r,
    lo_s,
    lo_r,
    to_s,
    to_r,
    st_s,
    st_r,
    ho_s,
    ho_r,
):
    me = lax.axis_index("tp")
    sp = lax.axis_index("sp")
    hk = heads * DK
    hv = heads * dv
    model = n * feats
    mine = pl.ds(pl.multiple_of(me * feats, feats), feats)

    loads = []

    def load(src, dst):
        copy = pltpu.make_async_copy(src, dst, load_sem.at[len(loads)])
        loads.append(copy)
        copy.start()
        return copy

    first = [
        load(conditioning, cond_v.at[0]),
        load(prompt, cond_v.at[1]),
        load(shift_m, mod_w.at[0]),
        load(scale_m, mod_w.at[1]),
        load(gate_m, mod_w.at[2]),
    ]
    own_x = [
        load(latent, x_all.at[pl.ds(0, rows), mine]),
        load(context, x_all.at[pl.ds(rows, crows), mine]),
    ]
    weights = [
        load(query_m, proj_w.at[pl.ds(0, hk)]),
        load(key_m, proj_w.at[pl.ds(hk, hk)]),
        load(value_m, proj_w.at[pl.ds(2 * hk, hv)]),
        load(og_m, proj_w.at[pl.ds(2 * hk + hv, hv)]),
        load(down, down_v),
    ]
    head_cols = pl.ds(pl.multiple_of(me * hk, hk), hk)
    small = [
        load(up.at[:, :, head_cols], up_v),
        load(bias.at[:, head_cols], bias_v),
        load(spike, spike_v),
        load(gain, gain_v),
    ]
    last = load(out_m, out_w)

    barrier = pltpu.get_barrier_semaphore()
    for d in range(1, n):
        pl.semaphore_signal(
            barrier, inc=1, device_id={"tp": lax.rem(me + d, n)}, device_id_type=MESH
        )
    for d in range(1, s):
        pl.semaphore_signal(
            barrier, inc=1, device_id={"sp": lax.rem(sp + d, s)}, device_id_type=MESH
        )
    pl.semaphore_wait(barrier, n - 1 + s - 1)

    started = []

    def send(src, dst, send_sem, recv_sem, axis, d):
        index, count = (me, n) if axis == "tp" else (sp, s)
        copy = pltpu.make_async_remote_copy(
            src_ref=src,
            dst_ref=dst,
            send_sem=send_sem.at[d - 1],
            recv_sem=recv_sem.at[d - 1],
            device_id={axis: lax.rem(index + d, count)},
            device_id_type=MESH,
        )
        copy.start()
        started.append(copy)
        return copy

    lat_copies, ctx_copies = {}, {}
    for d in range(1, n):
        lat_copies[d] = send(
            latent, x_all.at[pl.ds(0, rows), mine], lat_s, lat_r, "tp", d
        )
        ctx_copies[d] = send(
            context, x_all.at[pl.ds(rows, crows), mine], ctx_s, ctx_r, "tp", d
        )

    for copy in first:
        copy.wait()
    row_of = lax.broadcasted_iota(jnp.int32, (16, cond_v.shape[2]), 0)
    conds = jnp.where(
        row_of == 0, cond_v[0].astype(jnp.float32), cond_v[1].astype(jnp.float32)
    )
    conds = short(conds * lax.logistic(conds))
    for which in range(3):
        mod_own[2 * which : 2 * which + 2, :] = nt(conds, mod_w[which])[0:2]
    mod_own[6:8, :] = jnp.zeros((2, feats), jnp.float32)
    m1 = {
        d: send(mod_own, mod_recv.at[d - 1], m1_s, m1_r, "sp", d) for d in range(1, s)
    }

    for copy in own_x:
        copy.wait()

    def stats(columns):
        block = x_all[:, columns].astype(jnp.float32)
        return jnp.sum(block, axis=1, keepdims=True), jnp.sum(block * block, axis=1, keepdims=True)

    row_sum, row_squares = stats(mine)

    for d in range(1, s):
        m1[d].wait_recv()
    total = mod_own[...]
    for d in range(1, s):
        total = total + mod_recv[d - 1]
    mod_all[:, mine] = total
    m2 = {
        d: send(mod_all.at[:, mine], mod_all.at[:, mine], m2_s, m2_r, "tp", d)
        for d in range(1, n)
    }
    for d in range(1, n):
        lat_copies[d].wait_recv()
        ctx_copies[d].wait_recv()
        source = lax.rem(me - d + n, n)
        a, b = stats(pl.ds(pl.multiple_of(source * feats, feats), feats))
        row_sum, row_squares = row_sum + a, row_squares + b
    mean = row_sum / model
    spread = lax.rsqrt(row_squares / model - mean * mean + epsilon)
    for d in range(1, n):
        m2[d].wait_recv()
    for block in range(n):
        cols = slice(block * feats, (block + 1) * feats)
        x = (x_all[:, cols].astype(jnp.float32) - mean) * spread
        mod = mod_all[:, cols]
        xn[0:rows, cols] = short(x[0:rows] * (1.0 + mod[2:3]) + mod[0:1])
        xn[rows:, cols] = short(x[rows:] * (1.0 + mod[3:4]) + mod[1:2])

    for copy in weights:
        copy.wait()
    tile = min(256, hk)

    def project(t):
        cols = pl.ds(pl.multiple_of(t * tile, tile), tile)
        proj[:, cols] = short(nt(xn[...], proj_w[cols, :]))

    def project_range(begin, end):
        @pl.loop(begin // tile, end // tile)
        def _(t):
            project(t)

    project_range(hk, 2 * hk + hv)
    low = [nn(xn[...], down_v[direction]) for direction in range(2)]

    own_ctx = pl.ds(pl.multiple_of(sp * crows, crows), crows)
    ctx_kv[own_ctx, :] = proj[rows:, hk : 2 * hk + hv]
    ctx_low[own_ctx, :] = jnp.zeros((crows, ctx_low.shape[1]), jnp.float32)
    for direction in range(2):
        ctx_low[own_ctx, direction * 128 : direction * 128 + DECAY_RANK] = low[direction][rows:]
    kv = {
        d: send(ctx_kv.at[own_ctx], ctx_kv.at[own_ctx], kv_s, kv_r, "sp", d)
        for d in range(1, s)
    }
    lo = {
        d: send(ctx_low.at[own_ctx], ctx_low.at[own_ctx], lo_s, lo_r, "sp", d)
        for d in range(1, s)
    }

    for copy in small:
        copy.wait()
    head_lane = lax.broadcasted_iota(jnp.int32, (rows, spike_v.shape[2]), 1)
    ups = [up_v[direction].astype(jnp.float32) for direction in range(2)]
    cum = []
    for direction in range(2):
        logs = log_decay_of(low[direction][0:rows], ups[direction], bias_v[direction : direction + 1])
        added = [
            jnp.broadcast_to(
                jnp.sum(
                    jnp.where(head_lane == me * heads + h, spike_v[direction], 0.0),
                    axis=1,
                    keepdims=True,
                ),
                (rows, DK),
            )
            for h in range(heads)
        ]
        logs = logs + jnp.concatenate(added, axis=1)
        cum.append(exact(triangle_of(rows, direction == 1).astype(jnp.float32), logs))
    whole = [cum[0][rows - 1 : rows], cum[1][0:1]]
    tot_own[0:1, :] = whole[0]
    tot_own[1:2, :] = whole[1]
    tot_own[2:8, :] = jnp.zeros((6, hk), jnp.float32)
    to = {d: send(tot_own, tot_recv.at[d - 1], to_s, to_r, "sp", d) for d in range(1, s)}

    keys = proj[0:rows, hk : 2 * hk].astype(jnp.float32)
    for direction in range(2):
        weighted = short(keys * jnp.exp(whole[direction] - cum[direction]))
        for h in range(heads):
            st_own[direction, h * DK : (h + 1) * DK, :] = short(
                tn(
                    weighted[:, h * DK : (h + 1) * DK],
                    proj[0:rows, 2 * hk + h * dv : 2 * hk + (h + 1) * dv],
                )
            )
    st = {}
    for d in range(1, s):
        later = lax.rem(sp + d, s) > sp
        st[d] = send(
            st_own.at[jnp.where(later, 0, 1)], st_recv.at[d - 1], st_s, st_r, "sp", d
        )

    project_range(0, hk)
    project_range(2 * hk + hv, 2 * hk + 2 * hv)

    queries = proj[0:rows, 0:hk].astype(jnp.float32) * DK ** (-0.5)
    blocks = rows // BLK

    def span(b):
        return slice(b * BLK, (b + 1) * BLK)

    inside = [[], []]
    for b in range(blocks):
        f = cum[0][span(b)]
        inside[0].append(f if b == 0 else f - cum[0][b * BLK - 1 : b * BLK])
        f = cum[1][span(b)]
        inside[1].append(
            f if b == blocks - 1 else f - cum[1][(b + 1) * BLK : (b + 1) * BLK + 1]
        )
    ends = [[part[BLK - 1 : BLK] for part in inside[0]], [part[0:1] for part in inside[1]]]
    q_dec = [[short(queries[span(b)] * jnp.exp(inside[e][b])) for b in range(blocks)] for e in range(2)]
    k_dec = [[short(keys[span(b)] * jnp.exp(-inside[e][b])) for b in range(blocks)] for e in range(2)]
    k_end = [
        [short(keys[span(b)] * jnp.exp(ends[e][b] - inside[e][b])) for b in range(blocks)]
        for e in range(2)
    ]
    lower, upper = triangle_of(BLK, False), triangle_of(BLK, True)
    for h in range(heads):
        ch = slice(h * DK, (h + 1) * DK)
        lines = []
        for b in range(blocks):
            line = []
            for c in range(blocks):
                if b == c:
                    line.append(
                        jnp.where(lower, nt(q_dec[0][b][:, ch], k_dec[0][b][:, ch]), 0.0)
                        + jnp.where(upper, nt(q_dec[1][b][:, ch], k_dec[1][b][:, ch]), 0.0)
                    )
                    continue
                e = 0 if c < b else 1
                near = q_dec[e][b][:, ch]
                between = range(c + 1, b) if c < b else range(b + 1, c)
                if len(between) > 0:
                    gap = sum(ends[e][m][:, ch] for m in between)
                    near = short(queries[span(b)][:, ch] * jnp.exp(inside[e][b][:, ch] + gap))
                line.append(nt(near, k_end[e][c][:, ch]))
            lines.append(jnp.concatenate(line, axis=1) if blocks > 1 else line[0])
        scores = short(jnp.concatenate(lines, axis=0) if blocks > 1 else lines[0])
        local_out[:, h * dv : (h + 1) * dv] = nn(
            scores, proj[0:rows, 2 * hk + h * dv : 2 * hk + (h + 1) * dv]
        )

    for d in range(1, s):
        kv[d].wait_recv()
        lo[d].wait_recv()
    ctx_keys = ctx_kv[:, 0:hk].astype(jnp.float32)
    ctx_states = []
    for direction in range(2):
        logs = log_decay_of(
            ctx_low[:, direction * 128 : direction * 128 + DECAY_RANK],
            ups[direction],
            bias_v[direction : direction + 1],
        )
        length = s * crows
        c = exact(triangle_of(length, direction == 1).astype(jnp.float32), logs)
        end = c[length - 1 : length] if direction == 0 else c[0:1]
        weighted = short(ctx_keys * jnp.exp(end - c))
        ctx_states.append(
            [
                short(
                    tn(
                        weighted[:, h * DK : (h + 1) * DK],
                        ctx_kv[:, hk + h * dv : hk + (h + 1) * dv],
                    )
                )
                for h in range(heads)
            ]
        )

    for d in range(1, s):
        to[d].wait_recv()
    places = {d: lax.rem(sp - d + s, s) for d in range(1, s)}

    def passed(low_end, high_end, direction):
        result = jnp.zeros((1, hk), jnp.float32)
        for d in range(1, s):
            held = jnp.where((places[d] > low_end) & (places[d] < high_end), 1.0, 0.0)
            result = result + held * tot_recv[d - 1][direction : direction + 1]
        return result

    ctx_reach = [
        short(queries * jnp.exp(cum[0] + passed(-1, sp, 0))),
        short(queries * jnp.exp(cum[1] + passed(sp, s, 1))),
    ]
    for h in range(heads):
        ch = slice(h * DK, (h + 1) * DK)
        local_out[:, h * dv : (h + 1) * dv] += nn(
            jnp.concatenate([r[:, ch] for r in ctx_reach], axis=1),
            jnp.concatenate([ctx_states[e][h] for e in range(2)], axis=0),
        )
    reach = []
    for d in range(1, s):
        p = places[d]
        before = jnp.where(p < sp, 1.0, 0.0)
        exponent = before * (cum[0] + passed(p, sp, 0)) + (1.0 - before) * (
            cum[1] + passed(sp, p, 1)
        )
        reach.append(short(queries * jnp.exp(exponent)))
    gate_rows = proj[0:rows, 2 * hk + hv :].astype(jnp.float32)
    small_gate = gate_rows * lax.logistic(gate_rows) * gain_v[...]
    gi = lax.broadcasted_iota(jnp.int32, (dv, dv), 0) // VGROUP
    gj = lax.broadcasted_iota(jnp.int32, (dv, dv), 1) // VGROUP
    group = jnp.where(gi == gj, 1.0, 0.0).astype(jnp.bfloat16)
    for d in range(1, s):
        st[d].wait_recv()
    for h in range(heads):
        ch = slice(h * DK, (h + 1) * DK)
        vc = slice(h * dv, (h + 1) * dv)
        o = local_out[:, vc]
        for d in range(1, s):
            o = o + nn(reach[d - 1][:, ch], st_recv[d - 1, ch, :])
        squares = o * o
        top = short(squares)
        rest = short(squares - top.astype(jnp.float32))
        power = (nn(top, group) + nn(rest, group)) * (1.0 / VGROUP)
        ho_all[me, :, vc] = short(o * lax.rsqrt(power + epsilon) * small_gate[:, vc])

    ho = {d: send(ho_all.at[me], ho_all.at[me], ho_s, ho_r, "tp", d) for d in range(1, n)}
    last.wait()
    branch = nt(ho_all[me], out_w[:, mine])
    for d in range(1, n):
        ho[d].wait_recv()
        source = lax.rem(me - d + n, n)
        branch = branch + nt(
            ho_all[source], out_w[:, pl.ds(pl.multiple_of(source * feats, feats), feats)]
        )
    gates = mod_all[:, mine][4:5]
    out_ref[...] = short(x_all[0:rows, mine].astype(jnp.float32) + gates * branch)
    for copy in started:
        copy.wait_send()


def one_kernel(
    latent,
    context,
    conditioning,
    context_prompt_vector,
    shift_matrix,
    scale_matrix,
    residual_gate_matrix,
    query_matrix,
    key_matrix,
    value_matrix,
    gate_matrix,
    decay_down_factor,
    decay_up_factor,
    decay_key_bias,
    spike_log_decay,
    output_gain,
    output_matrix,
):
    n, s = lax.axis_size("tp"), lax.axis_size("sp")
    rows, feats = latent.shape
    crows = context.shape[0]
    heads = HEADS // n
    hk, hv = query_matrix.shape[0], value_matrix.shape[0]
    dv = hv // heads
    model = n * feats
    both = rows + crows
    inputs = conditioning.shape[0]
    bf, f32 = jnp.bfloat16, jnp.float32
    vmem, dma = pltpu.VMEM, pltpu.SemaphoreType.DMA
    pair = lambda k: [dma((k,)), dma((k,))]
    scratch = [
        vmem((both, model), bf),
        vmem((both, model), bf),
        vmem((3, feats, inputs), bf),
        vmem((2 * hk + 2 * hv, model), bf),
        vmem((output_matrix.shape[0], model), bf),
        vmem((2, model, DECAY_RANK), bf),
        vmem((2, DECAY_RANK, hk), bf),
        vmem((2, hk), f32),
        vmem(spike_log_decay.shape, f32),
        vmem((1, hv), f32),
        vmem((2, 1, inputs), bf),
        vmem((8, feats), f32),
        vmem((s - 1, 8, feats), f32),
        vmem((8, model), f32),
        vmem((both, 2 * hk + 2 * hv), bf),
        vmem((s * crows, hk + hv), bf),
        vmem((s * crows, 256), f32),
        vmem((8, hk), f32),
        vmem((s - 1, 8, hk), f32),
        vmem((2, hk, dv), bf),
        vmem((s - 1, hk, dv), bf),
        vmem((rows, hv), f32),
        vmem((n, rows, hv), bf),
        dma((17,)),
    ]
    for count in (n - 1, n - 1, s - 1, n - 1, s - 1, s - 1, s - 1, s - 1, n - 1):
        scratch += pair(count)
    return pl.pallas_call(
        functools.partial(layer_kernel, n, s, rows, crows, feats, heads, dv),
        out_shape=jax.ShapeDtypeStruct((rows, feats), bf),
        in_specs=[pl.BlockSpec(memory_space=pl.ANY)] * 17,
        out_specs=pl.BlockSpec(memory_space=pltpu.VMEM),
        scratch_shapes=scratch,
        compiler_params=pltpu.CompilerParams(
            collective_id=0, has_side_effects=True, vmem_limit_bytes=60 * 1024 * 1024
        ),
        name="layer",
    )(
        latent,
        context,
        conditioning.reshape(1, -1),
        context_prompt_vector.reshape(1, -1),
        shift_matrix,
        scale_matrix,
        residual_gate_matrix,
        query_matrix,
        key_matrix,
        value_matrix,
        gate_matrix,
        decay_down_factor,
        decay_up_factor,
        decay_key_bias,
        spike_log_decay,
        output_gain.reshape(1, -1),
        output_matrix,
    )


def solution(mesh):
    placed = (
        P("sp", "tp"),
        P("sp", "tp"),
        P("sp"),
        P("sp"),
        P("tp", "sp"),
        P("tp", "sp"),
        P("tp", "sp"),
        P("tp", None),
        P("tp", None),
        P("tp", None),
        P("tp", None),
        P(),
        P(),
        P(),
        P(None, "sp", None),
        P("tp"),
        P("tp", None),
    )
    whole_heads = HEADS % mesh.shape["tp"] == 0
    return jax.shard_map(
        one_kernel if whole_heads else local, mesh=mesh, in_specs=placed, out_specs=P("sp", "tp"), check_vma=False
    )
```

```python
import functools

import jax
import jax.numpy as jnp
from jax import lax
from jax.experimental import pallas as pl
from jax.experimental.pallas import tpu as pltpu
from jax.sharding import PartitionSpec as P

D = 4096
HEADS = 16
DK = 128
DECAY_RANK = 16
BLK = 64
VGROUP = 64
MESH = pl.DeviceIdType.MESH


epsilon = 1e-05
gate_norm = 16.0
precise = lax.Precision.HIGHEST


def for_sending(value):

    def short(part):
        return part.astype(jnp.bfloat16) if part.dtype == jnp.float32 else part

    return jax.tree.map(short, value)


def from_partner(value, axis, distance):
    return lax.ppermute(value, axis, [(i, i ^ 1 << distance) for i in range(lax.axis_size(axis))])


def carried_in(value, axis, combine, identity, reverse):
    peers, index = (lax.axis_size(axis), lax.axis_index(axis))
    everything = jax.tree.map(
        lambda part, kind: lax.all_gather(part.astype(kind), axis),
        value,
        (jnp.bfloat16, jnp.bfloat16),
    )
    start = jax.tree.map(
        lambda part, zero: jnp.broadcast_to(jnp.asarray(zero, part.dtype), part.shape),
        value,
        identity,
    )

    def turn(k, before):
        at = peers - 1 - k if reverse else k
        reached = at > index if reverse else at < index
        new = combine(
            before, jax.tree.map(lambda part, own: part[at].astype(own.dtype), everything, value)
        )
        return jax.tree.map(lambda a, b: jnp.where(reached, a, b), new, before)

    return lax.fori_loop(0, peers, turn, start)


def linear(rows, weight):
    return lax.dot_general(
        rows, weight, (((1,), (1,)), ((), ())), preferred_element_type=jnp.float32
    )


def modulated(rows, row_sum, row_squares, shift_vec, scale_vec):
    rows_f = rows.astype(jnp.float32)
    mean_val = row_sum / D
    variance = row_squares / D - mean_val * mean_val
    return (
        (rows_f - mean_val) * lax.rsqrt(variance + epsilon) * (1.0 + scale_vec) + shift_vec
    ).astype(jnp.bfloat16)


def reverse_rows(array):
    return jnp.flip(array, axis=0)


def end_state(key_rows, value_rows, log_decay):
    cumulative = jnp.cumsum(log_decay, axis=0)
    totals = cumulative[-1]
    weighted = key_rows * jnp.exp(totals - cumulative)
    return (jnp.exp(totals), jnp.einsum("nhd,nhe->hde", weighted, value_rows, precision=precise))


def combine(earlier, later):
    return (earlier[0] * later[0], later[0][..., None] * earlier[1] + later[1])


def blockwise(queries, key_rows, value_rows, log_decay, carried, block_len):
    length, head_count, _ = queries.shape
    value_width = value_rows.shape[-1]
    blocks = length // block_len

    def shaped(array):
        return array.reshape(blocks, block_len, head_count, array.shape[-1])

    triangle = jnp.tril(jnp.ones((block_len, block_len), jnp.float32))

    def advance(state_now, inputs):
        block_q, block_k, block_v, block_a = inputs
        cumulative = jnp.cumsum(block_a, axis=0)
        block_end = cumulative[-1]
        query_dec = block_q * jnp.exp(cumulative)
        scores = (
            jnp.einsum("ihd,jhd->hij", query_dec, block_k * jnp.exp(-cumulative), precision=precise)
            * triangle
        )
        result = jnp.einsum("hij,jhe->ihe", scores, block_v, precision=precise)
        result = result + jnp.einsum("ihd,hde->ihe", query_dec, state_now, precision=precise)
        state_next = state_now * jnp.exp(block_end)[:, :, None] + jnp.einsum(
            "jhd,jhe->hde", block_k * jnp.exp(block_end - cumulative), block_v, precision=precise
        )
        return (state_next, result)

    _, outputs = lax.scan(
        advance, carried, (shaped(queries), shaped(key_rows), shaped(value_rows), shaped(log_decay))
    )
    return outputs.reshape(length, head_count, value_width)


def head_channels(pieces, per_head, tp_index):
    for bit_number in range(per_head.bit_length() - 1):
        partner = from_partner(
            (for_sending(pieces[0]), for_sending(pieces[1]), for_sending(pieces[2])),
            "tp",
            bit_number,
        )
        upper = tp_index // (1 << bit_number) % 2 == 1
        pieces = tuple(
            (
                jnp.where(
                    upper,
                    jnp.concatenate([theirs, mine], axis=1),
                    jnp.concatenate([mine, theirs], axis=1),
                )
                for mine, theirs in zip(pieces, partner)
            )
        )
    return pieces


def context_totals(fwd_growth, fwd_state, bwd_growth, bwd_state, identity):

    def absorb(carried, piece):
        return (combine(carried, piece), None)

    total_fwd, _ = lax.scan(absorb, identity, (fwd_growth, fwd_state))
    total_bwd, _ = lax.scan(absorb, identity, (bwd_growth, bwd_state), reverse=True)
    return (total_fwd, total_bwd)


def stored(array):
    return lax.optimization_barrier(array.astype(jnp.bfloat16))


def local(
    latent,
    context,
    conditioning,
    context_prompt_vector,
    shift_matrix,
    scale_matrix,
    residual_gate_matrix,
    query_matrix,
    key_matrix,
    value_matrix,
    gate_matrix,
    decay_down_factor,
    decay_up_factor,
    decay_key_bias,
    spike_log_decay,
    output_gain,
    output_matrix,
):
    tp_count = lax.axis_size("tp")
    tp_index = lax.axis_index("tp")
    per_head = max(tp_count // HEADS, 1)
    heads_per_shard = max(HEADS // tp_count, 1)
    leading_head = tp_index // per_head * heads_per_shard
    tok_rows = latent.shape[0]
    conds = jax.nn.silu(
        jnp.stack([conditioning, context_prompt_vector]).astype(jnp.float32)
    ).astype(jnp.bfloat16)
    shifts, scales, gates = lax.psum(
        (
            linear(conds, shift_matrix),
            linear(conds, scale_matrix),
            linear(conds, residual_gate_matrix),
        ),
        "sp",
    )
    down_both = jnp.concatenate([decay_down_factor[0].T, decay_down_factor[1].T], axis=0)
    lat_weights = (query_matrix, key_matrix, value_matrix, gate_matrix, down_both)
    ctx_weights = (key_matrix, value_matrix, down_both)
    lat_f = latent.astype(jnp.float32)
    ctx_f = context.astype(jnp.float32)
    lat_sum, lat_squares, ctx_sum, ctx_squares = lax.psum(
        (
            jnp.sum(lat_f, axis=1, keepdims=True),
            jnp.sum(lat_f * lat_f, axis=1, keepdims=True),
            jnp.sum(ctx_f, axis=1, keepdims=True),
            jnp.sum(ctx_f * ctx_f, axis=1, keepdims=True),
        ),
        "tp",
    )
    latent_normalized = modulated(latent, lat_sum, lat_squares, shifts[0], scales[0])
    normed_ctx = modulated(context, ctx_sum, ctx_squares, shifts[1], scales[1])
    lat_piece = lax.all_gather(latent_normalized, "tp", axis=1, tiled=True)
    ctx_piece = lax.all_gather(normed_ctx, "tp", axis=1, tiled=True)
    lat_new = tuple((linear(lat_piece, weight) for weight in lat_weights))
    ctx_new = tuple((linear(ctx_piece, weight) for weight in ctx_weights))
    query_part, key_part, value_part, gate_part, low_rank_part = lat_new
    ctx_key_part, ctx_value_part, ctx_low = ctx_new
    query_full, key_full, ctx_key_full = head_channels(
        (stored(query_part), stored(key_part), stored(ctx_key_part)), per_head, tp_index
    )

    def split_heads(rows, width):
        return rows.astype(jnp.float32).reshape(rows.shape[0], heads_per_shard, width)

    value_cols = value_part.shape[1] // heads_per_shard
    queries = split_heads(query_full, DK) * DK ** (-0.5)
    key_rows = split_heads(key_full, DK)
    ctx_keys = split_heads(ctx_key_full, DK)
    values_lat = split_heads(stored(value_part), value_cols)
    values_ctx = split_heads(stored(ctx_value_part), value_cols)
    gate_rows = stored(gate_part).astype(jnp.float32)

    def per_head_decay(low_rows, direction):
        up_part = lax.dynamic_slice_in_dim(
            decay_up_factor[direction], leading_head * DK, heads_per_shard * DK, 1
        ).astype(jnp.float32)
        bias_part = lax.dynamic_slice_in_dim(
            decay_key_bias[direction], leading_head * DK, heads_per_shard * DK, 0
        )
        pre_act = jnp.dot(low_rows, up_part, precision=precise) + bias_part
        return (jax.nn.log_sigmoid(pre_act) / gate_norm).reshape(
            low_rows.shape[0], heads_per_shard, DK
        )

    decay_spikes = lax.dynamic_slice_in_dim(spike_log_decay, leading_head, heads_per_shard, 2)
    latent_forward = per_head_decay(low_rank_part[:, :DECAY_RANK], 0) + decay_spikes[0][:, :, None]
    latent_backward = per_head_decay(low_rank_part[:, DECAY_RANK:], 1) + decay_spikes[1][:, :, None]
    ctx_fwd = per_head_decay(ctx_low[:, :DECAY_RANK], 0)
    ctx_bwd = per_head_decay(ctx_low[:, DECAY_RANK:], 1)
    cf_growth, cf_state = end_state(ctx_keys, values_ctx, ctx_fwd)
    cb_growth, cb_state = end_state(
        reverse_rows(ctx_keys), reverse_rows(values_ctx), reverse_rows(ctx_bwd)
    )
    lf_growth, lf_state = end_state(key_rows, values_lat, latent_forward)
    lb_growth, lb_state = end_state(
        reverse_rows(key_rows), reverse_rows(values_lat), reverse_rows(latent_backward)
    )
    identity = (
        jnp.ones((heads_per_shard, DK), jnp.float32),
        jnp.zeros((heads_per_shard, DK, value_cols), jnp.float32),
    )
    ctx_gathered = (
        lax.all_gather(cf_growth[None].astype(jnp.bfloat16), "sp", axis=0, tiled=True).astype(
            jnp.float32
        ),
        lax.all_gather(cf_state[None].astype(jnp.bfloat16), "sp", axis=0, tiled=True).astype(
            jnp.float32
        ),
        lax.all_gather(cb_growth[None].astype(jnp.bfloat16), "sp", axis=0, tiled=True).astype(
            jnp.float32
        ),
        lax.all_gather(cb_state[None].astype(jnp.bfloat16), "sp", axis=0, tiled=True).astype(
            jnp.float32
        ),
    )
    total_fwd, total_bwd = context_totals(
        ctx_gathered[0], ctx_gathered[1], ctx_gathered[2], ctx_gathered[3], identity
    )
    prefix = carried_in((lf_growth, lf_state), "sp", combine, identity, False)
    suffix = carried_in((lb_growth, lb_state), "sp", combine, identity, True)
    start_fwd = combine(total_fwd, prefix)[1]
    start_bwd = combine(total_bwd, suffix)[1]
    zero_state = jnp.zeros((heads_per_shard, DK, value_cols), jnp.float32)

    def direction_out(query_rows, key_list, value_list, log_decay, start_state):
        local_part = blockwise(query_rows, key_list, value_list, log_decay, zero_state, BLK)
        reach = query_rows * jnp.exp(jnp.cumsum(log_decay, axis=0))
        return local_part + jnp.einsum("nhd,hde->nhe", reach, start_state, precision=precise)

    out_fwd = direction_out(queries, key_rows, values_lat, latent_forward, start_fwd)
    out_bwd = reverse_rows(
        direction_out(
            reverse_rows(queries),
            reverse_rows(key_rows),
            reverse_rows(values_lat),
            reverse_rows(latent_backward),
            start_bwd,
        )
    )
    grouped = (out_fwd + out_bwd).reshape(tok_rows, -1, VGROUP)
    grouped = grouped * lax.rsqrt(jnp.mean(grouped * grouped, axis=-1, keepdims=True) + epsilon)
    heads_out = (grouped.reshape(tok_rows, -1) * output_gain * jax.nn.silu(gate_rows)).astype(
        jnp.bfloat16
    )
    branch = linear(lax.all_gather(heads_out, "tp", axis=1, tiled=True), output_matrix)
    return (latent.astype(jnp.float32) + gates[0] * branch).astype(jnp.bfloat16)


def exact(a, b):
    return lax.dot_general(
        a, b, (((1,), (0,)), ((), ())), precision=precise, preferred_element_type=jnp.float32
    )


def nt(a, b):
    return lax.dot_general(a, b, (((1,), (1,)), ((), ())), preferred_element_type=jnp.float32)


def nn(a, b):
    return lax.dot_general(a, b, (((1,), (0,)), ((), ())), preferred_element_type=jnp.float32)


def tn(a, b):
    return lax.dot_general(a, b, (((0,), (0,)), ((), ())), preferred_element_type=jnp.float32)


def short(value):
    return value.astype(jnp.bfloat16)


def log_decay_of(low, up, bias):
    pre = exact(low, up) + bias
    return (jnp.minimum(pre, 0.0) - jnp.log1p(jnp.exp(-jnp.abs(pre)))) / gate_norm


def triangle_of(size, upper):
    i = lax.broadcasted_iota(jnp.int32, (size, size), 0)
    j = lax.broadcasted_iota(jnp.int32, (size, size), 1)
    return (j >= i) if upper else (j <= i)


def layer_kernel(
    n,
    s,
    inner,
    rows,
    crows,
    feats,
    heads,
    dv,
    latent,
    context,
    conditioning,
    prompt,
    shift_m,
    scale_m,
    gate_m,
    query_m,
    key_m,
    value_m,
    og_m,
    down,
    up,
    bias,
    spike,
    gain,
    out_m,
    out_ref,
    x_all,
    xn,
    acc,
    low_acc,
    mod_w,
    proj_w,
    out_w,
    down_v,
    up_v,
    bias_v,
    spike_v,
    gain_v,
    cond_v,
    mod_own,
    mod_recv,
    mod_all,
    proj,
    ctx_kv,
    ctx_low,
    tot_own,
    tot_recv,
    st_own,
    st_recv,
    local_out,
    ho_all,
    load_sem,
    xs_up,
    xr_up,
    xs_dn,
    xr_dn,
    xs_y,
    xr_y,
    m1_s,
    m1_r,
    m2_s,
    m2_r,
    kv_s,
    kv_r,
    lo_s,
    lo_r,
    to_s,
    to_r,
    st_s,
    st_r,
    hs_up,
    hr_up,
    hs_dn,
    hr_dn,
    hs_y,
    hr_y,
):
    me = lax.axis_index("tp")
    sp = lax.axis_index("sp")
    hk = heads * DK
    hv = heads * dv
    model = n * feats
    mine = pl.ds(pl.multiple_of(me * feats, feats), feats)

    loads = []

    def load(src, dst):
        copy = pltpu.make_async_copy(src, dst, load_sem.at[len(loads)])
        loads.append(copy)
        copy.start()
        return copy

    first = [
        load(conditioning, cond_v.at[0]),
        load(prompt, cond_v.at[1]),
        load(shift_m, mod_w.at[0]),
        load(scale_m, mod_w.at[1]),
        load(gate_m, mod_w.at[2]),
    ]
    own_x = [
        load(latent, x_all.at[pl.ds(0, rows), mine]),
        load(context, x_all.at[pl.ds(rows, crows), mine]),
    ]
    weights = [
        load(query_m, proj_w.at[pl.ds(0, hk)]),
        load(key_m, proj_w.at[pl.ds(hk, hk)]),
        load(value_m, proj_w.at[pl.ds(2 * hk, hv)]),
        load(og_m, proj_w.at[pl.ds(2 * hk + hv, hv)]),
        load(down, down_v),
    ]
    head_cols = pl.ds(pl.multiple_of(me * hk, hk), hk)
    small = [
        load(up.at[:, :, head_cols], up_v),
        load(bias.at[:, head_cols], bias_v),
        load(spike, spike_v),
        load(gain, gain_v),
    ]
    last = load(out_m, out_w)

    barrier = pltpu.get_barrier_semaphore()
    for d in range(1, n):
        pl.semaphore_signal(
            barrier, inc=1, device_id={"tp": lax.rem(me + d, n)}, device_id_type=MESH
        )
    for d in range(1, s):
        pl.semaphore_signal(
            barrier, inc=1, device_id={"sp": lax.rem(sp + d, s)}, device_id_type=MESH
        )
    pl.semaphore_wait(barrier, n - 1 + s - 1)

    started = []

    def send(src, dst, send_sem, recv_sem, axis, d):
        index, count = (me, n) if axis == "tp" else (sp, s)
        copy = pltpu.make_async_remote_copy(
            src_ref=src,
            dst_ref=dst,
            send_sem=send_sem.at[d - 1],
            recv_sem=recv_sem.at[d - 1],
            device_id={axis: lax.rem(index + d, count)},
            device_id_type=MESH,
        )
        copy.start()
        started.append(copy)
        return copy

    line = n // inner
    z, y = lax.div(me, inner), lax.rem(me, inner)

    def block_of(at, column):
        return at * inner + column

    class Gather:
        def __init__(self, view, pieces, up, down, across):
            self.view, self.pieces = view, pieces
            self.lanes = {"up": up, "down": down, "across": across}

        def copy(self, lane, block, piece, slot, target):
            sends, recvs = self.lanes[lane]
            ref = self.view(block, piece)
            return pltpu.make_async_remote_copy(
                src_ref=ref,
                dst_ref=ref,
                send_sem=sends.at[slot, piece],
                recv_sem=recvs.at[slot, piece],
                device_id={"tp": target},
                device_id_type=MESH,
            )

        def hop(self, lane, at, piece, slot):
            target = {
                "up": block_of(jnp.minimum(z + 1, line - 1), y),
                "down": block_of(jnp.maximum(z - 1, 0), y),
                "across": block_of(z, inner - 1 - y),
            }[lane]
            return self.copy(lane, block_of(at, y), piece, slot, target)

        def sends(self, k, piece, act):
            for lane, at, has, onward, slot in (
                ("up", z - k, z >= k, z + 1 < line, max(2 * k - 1, 0)),
                ("down", z + k, z + k < line, z > 0, 2 * k),
            ):
                if k < line - 1:
                    pl.when(has & onward)(lambda: act(self.hop(lane, at, piece, k)))
                if inner > 1 and (k > 0 or lane == "up"):
                    pl.when(has)(lambda: act(self.hop("across", at, piece, slot)))

        def start(self):
            for piece in range(self.pieces):
                self.sends(0, piece, lambda c: c.start())

        def step(self, k):
            for piece in range(self.pieces):
                for lane, at, has in (("up", z - k, z >= k), ("down", z + k, z + k < line)):
                    pl.when(has)(lambda: self.hop(lane, at, piece, k - 1).wait_recv())
                self.sends(k, piece, lambda c: c.start())

        def column(self, k, work):
            pl.when(z >= k)(lambda: work(block_of(z - k, y)))
            pl.when(z + k < line)(lambda: work(block_of(z + k, y)))

        def other(self, k, work):
            if inner == 1:
                return

            def arrive(at, slot):
                block = block_of(at, inner - 1 - y)
                for piece in range(self.pieces):
                    self.copy("across", block, piece, slot, block).wait_recv()
                work(block)

            if k == 0:
                arrive(z, 0)
                return
            pl.when(z >= k)(lambda: arrive(z - k, 2 * k - 1))
            pl.when(z + k < line)(lambda: arrive(z + k, 2 * k))

        def drain(self):
            for k in range(line):
                for piece in range(self.pieces):
                    self.sends(k, piece, lambda c: c.wait_send())

    both = rows + crows
    cut = both // 32 * 16

    def x_view(block, piece):
        part = pl.ds(0, cut) if piece == 0 else pl.ds(cut, both - cut)
        return x_all.at[part, pl.ds(pl.multiple_of(block * feats, feats), feats)]

    xg = Gather(x_view, 2, (xs_up, xr_up), (xs_dn, xr_dn), (xs_y, xr_y))
    for copy in own_x:
        copy.wait()
    xg.start()

    for copy in first:
        copy.wait()
    def one_row(which):
        part = cond_v[which].astype(jnp.float32)
        return jnp.concatenate([part[r : r + 1] for r in range(part.shape[0])], axis=1)

    row_of = lax.broadcasted_iota(jnp.int32, (16, shift_m.shape[1]), 0)
    conds = jnp.where(row_of == 0, one_row(0), one_row(1))
    conds = short(conds * lax.logistic(conds))
    for which in range(3):
        mod_own[2 * which : 2 * which + 2, :] = nt(conds, mod_w[which])[0:2]
    mod_own[6:8, :] = jnp.zeros((2, feats), jnp.float32)
    m1 = {
        d: send(mod_own, mod_recv.at[d - 1], m1_s, m1_r, "sp", d) for d in range(1, s)
    }

    own = x_all[:, mine]
    ones = jnp.ones((16, feats), jnp.bfloat16)
    own_f = own.astype(jnp.float32)
    rest = own_f * own_f
    row_squares = jnp.zeros((16, both), jnp.float32)
    for _ in range(3):
        top = short(rest)
        row_squares = row_squares + nt(ones, top)
        rest = rest - top.astype(jnp.float32)
    row_sum = nt(ones, own)

    if line > 1:
        xg.step(1)
    for d in range(1, s):
        m1[d].wait_recv()
    total = mod_own[...]
    for d in range(1, s):
        total = total + mod_recv[d - 1]
    mod_all[:, mine] = total
    stat_cols = pl.ds(pl.multiple_of(me * feats, feats), both)
    mod_all[6:7, stat_cols] = row_sum[0:1]
    mod_all[7:8, stat_cols] = row_squares[0:1]
    m2 = {
        d: send(mod_all.at[:, mine], mod_all.at[:, mine], m2_s, m2_r, "tp", d)
        for d in range(1, n)
    }
    tile = min(256, hk)
    columns = acc.shape[1]
    acc[...] = jnp.zeros(acc.shape, jnp.float32)
    low_acc[...] = jnp.zeros(low_acc.shape, jnp.float32)

    def moments():
        for d in range(1, n):
            m2[d].wait_recv()
        diagonal = lax.broadcasted_iota(jnp.int32, (both, both), 0) == lax.broadcasted_iota(
            jnp.int32, (both, both), 1
        )

        def column_of(row):
            whole_row = sum(mod_all[row : row + 1, b * feats : b * feats + both] for b in range(n))
            return jnp.sum(jnp.where(diagonal, whole_row, 0.0), axis=1, keepdims=True) / model

        mean = column_of(6)
        return mean, lax.rsqrt(column_of(7) - mean * mean + epsilon)

    def project_block(block, mean, spread):
        cols = pl.ds(pl.multiple_of(block * feats, feats), feats)
        x = (x_all[:, cols].astype(jnp.float32) - mean) * spread
        mod = mod_all[:, cols]
        xn[0:rows, :] = short(x[0:rows] * (1.0 + mod[2:3]) + mod[0:1])
        xn[rows:, :] = short(x[rows:] * (1.0 + mod[3:4]) + mod[1:2])
        low_acc[...] += nt(xn[...], down_v[:, cols])

        @pl.loop(0, columns // tile)
        def _(t):
            out = pl.ds(pl.multiple_of(t * tile, tile), tile)
            acc[:, out] += nt(xn[...], proj_w[out, cols])

    ready = None
    for k in range(2, line + 1):
        if k < line:
            xg.step(k)
        if ready is None:
            ready = moments()
            for copy in weights:
                copy.wait()
            work = lambda block: project_block(block, *ready)
            work(me)
        xg.column(k - 1, work)
        xg.other(k - 2, work)
    xg.other(line - 1, work)
    proj[...] = short(acc[...])

    own_ctx = pl.ds(pl.multiple_of(sp * crows, crows), crows)
    ctx_kv[own_ctx, :] = proj[rows:, hk : 2 * hk + hv]
    ctx_low[own_ctx, :] = jnp.zeros((crows, ctx_low.shape[1]), jnp.float32)
    ctx_low[own_ctx, 0 : 2 * DECAY_RANK] = low_acc[rows:]
    kv = {
        d: send(ctx_kv.at[own_ctx], ctx_kv.at[own_ctx], kv_s, kv_r, "sp", d)
        for d in range(1, s)
    }
    lo = {
        d: send(ctx_low.at[own_ctx], ctx_low.at[own_ctx], lo_s, lo_r, "sp", d)
        for d in range(1, s)
    }

    for copy in small:
        copy.wait()
    slot_head = lax.broadcasted_iota(jnp.int32, (spike_v.shape[1], hk), 0)
    lane_head = lax.broadcasted_iota(jnp.int32, (spike_v.shape[1], hk), 1) // DK
    pick = jnp.where(slot_head == me * heads + lane_head, 1.0, 0.0)
    none = jnp.zeros((DECAY_RANK, hk), jnp.float32)
    ups = [
        jnp.concatenate([up_v[0].astype(jnp.float32), none], axis=0),
        jnp.concatenate([none, up_v[1].astype(jnp.float32)], axis=0),
    ]
    cum = []
    for direction in range(2):
        logs = log_decay_of(low_acc[0:rows], ups[direction], bias_v[direction : direction + 1])
        logs = logs + lax.dot_general(
            spike_v[direction],
            pick,
            (((0,), (0,)), ((), ())),
            precision=precise,
            preferred_element_type=jnp.float32,
        )
        cum.append(exact(triangle_of(rows, direction == 1).astype(jnp.float32), logs))
    whole = [cum[0][rows - 1 : rows], cum[1][0:1]]
    tot_own[0:1, :] = whole[0]
    tot_own[1:2, :] = whole[1]
    tot_own[2:8, :] = jnp.zeros((6, hk), jnp.float32)
    to = {d: send(tot_own, tot_recv.at[d - 1], to_s, to_r, "sp", d) for d in range(1, s)}

    keys = proj[0:rows, hk : 2 * hk].astype(jnp.float32)
    for direction in range(2):
        weighted = short(keys * jnp.exp(whole[direction] - cum[direction]))
        for h in range(heads):
            st_own[direction, h * DK : (h + 1) * DK, :] = short(
                tn(
                    weighted[:, h * DK : (h + 1) * DK],
                    proj[0:rows, 2 * hk + h * dv : 2 * hk + (h + 1) * dv],
                )
            )
    st = {}
    for d in range(1, s):
        later = lax.rem(sp + d, s) > sp
        st[d] = send(
            st_own.at[jnp.where(later, 0, 1)], st_recv.at[d - 1], st_s, st_r, "sp", d
        )

    queries = proj[0:rows, 0:hk].astype(jnp.float32) * DK ** (-0.5)
    blocks = rows // BLK

    def span(b):
        return slice(b * BLK, (b + 1) * BLK)

    inside = [[], []]
    for b in range(blocks):
        f = cum[0][span(b)]
        inside[0].append(f if b == 0 else f - cum[0][b * BLK - 1 : b * BLK])
        f = cum[1][span(b)]
        inside[1].append(
            f if b == blocks - 1 else f - cum[1][(b + 1) * BLK : (b + 1) * BLK + 1]
        )
    ends = [[part[BLK - 1 : BLK] for part in inside[0]], [part[0:1] for part in inside[1]]]
    q_dec = [[short(queries[span(b)] * jnp.exp(inside[e][b])) for b in range(blocks)] for e in range(2)]
    k_dec = [[short(keys[span(b)] * jnp.exp(-inside[e][b])) for b in range(blocks)] for e in range(2)]
    k_end = [
        [short(keys[span(b)] * jnp.exp(ends[e][b] - inside[e][b])) for b in range(blocks)]
        for e in range(2)
    ]
    lower, upper = triangle_of(BLK, False), triangle_of(BLK, True)
    for h in range(heads):
        ch = slice(h * DK, (h + 1) * DK)
        lines = []
        for b in range(blocks):
            strip = []
            for c in range(blocks):
                if b == c:
                    strip.append(
                        jnp.where(lower, nt(q_dec[0][b][:, ch], k_dec[0][b][:, ch]), 0.0)
                        + jnp.where(upper, nt(q_dec[1][b][:, ch], k_dec[1][b][:, ch]), 0.0)
                    )
                    continue
                e = 0 if c < b else 1
                near = q_dec[e][b][:, ch]
                between = range(c + 1, b) if c < b else range(b + 1, c)
                if len(between) > 0:
                    gap = sum(ends[e][m][:, ch] for m in between)
                    near = short(queries[span(b)][:, ch] * jnp.exp(inside[e][b][:, ch] + gap))
                strip.append(nt(near, k_end[e][c][:, ch]))
            lines.append(jnp.concatenate(strip, axis=1) if blocks > 1 else strip[0])
        scores = short(jnp.concatenate(lines, axis=0) if blocks > 1 else lines[0])
        local_out[:, h * dv : (h + 1) * dv] = nn(
            scores, proj[0:rows, 2 * hk + h * dv : 2 * hk + (h + 1) * dv]
        )

    for d in range(1, s):
        kv[d].wait_recv()
        lo[d].wait_recv()
    ctx_keys = ctx_kv[:, 0:hk].astype(jnp.float32)
    ctx_states = []
    for direction in range(2):
        logs = log_decay_of(
            ctx_low[:, 0 : 2 * DECAY_RANK],
            ups[direction],
            bias_v[direction : direction + 1],
        )
        length = s * crows
        c = exact(triangle_of(length, direction == 1).astype(jnp.float32), logs)
        end = c[length - 1 : length] if direction == 0 else c[0:1]
        weighted = short(ctx_keys * jnp.exp(end - c))
        ctx_states.append(
            [
                short(
                    tn(
                        weighted[:, h * DK : (h + 1) * DK],
                        ctx_kv[:, hk + h * dv : hk + (h + 1) * dv],
                    )
                )
                for h in range(heads)
            ]
        )

    for d in range(1, s):
        to[d].wait_recv()
    places = {d: lax.rem(sp - d + s, s) for d in range(1, s)}

    def passed(low_end, high_end, direction):
        result = jnp.zeros((1, hk), jnp.float32)
        for d in range(1, s):
            held = jnp.where((places[d] > low_end) & (places[d] < high_end), 1.0, 0.0)
            result = result + held * tot_recv[d - 1][direction : direction + 1]
        return result

    ctx_reach = [
        short(queries * jnp.exp(cum[0] + passed(-1, sp, 0))),
        short(queries * jnp.exp(cum[1] + passed(sp, s, 1))),
    ]
    for h in range(heads):
        ch = slice(h * DK, (h + 1) * DK)
        local_out[:, h * dv : (h + 1) * dv] += nn(
            jnp.concatenate([r[:, ch] for r in ctx_reach], axis=1),
            jnp.concatenate([ctx_states[e][h] for e in range(2)], axis=0),
        )
    reach = []
    for d in range(1, s):
        p = places[d]
        before = jnp.where(p < sp, 1.0, 0.0)
        exponent = before * (cum[0] + passed(p, sp, 0)) + (1.0 - before) * (
            cum[1] + passed(sp, p, 1)
        )
        reach.append(short(queries * jnp.exp(exponent)))
    gate_rows = proj[0:rows, 2 * hk + hv :].astype(jnp.float32)
    small_gate = gate_rows * lax.logistic(gate_rows) * gain_v[...]
    gi = lax.broadcasted_iota(jnp.int32, (dv, dv), 0) // VGROUP
    gj = lax.broadcasted_iota(jnp.int32, (dv, dv), 1) // VGROUP
    group = jnp.where(gi == gj, 1.0, 0.0).astype(jnp.bfloat16)
    for d in range(1, s):
        st[d].wait_recv()
    for h in range(heads):
        ch = slice(h * DK, (h + 1) * DK)
        vc = slice(h * dv, (h + 1) * dv)
        o = local_out[:, vc]
        for d in range(1, s):
            o = o + nn(reach[d - 1][:, ch], st_recv[d - 1, ch, :])
        squares = o * o
        top = short(squares)
        rest = short(squares - top.astype(jnp.float32))
        power = (nn(top, group) + nn(rest, group)) * (1.0 / VGROUP)
        ho_all[me, :, vc] = short(o * lax.rsqrt(power + epsilon) * small_gate[:, vc])

    def ho_view(block, piece):
        return ho_all.at[block, pl.ds(piece * (rows // 2), rows // 2)]

    hg = Gather(ho_view, 2, (hs_up, hr_up), (hs_dn, hr_dn), (hs_y, hr_y))
    hg.start()
    last.wait()
    local_out[...] = nt(ho_all[me], out_w[:, mine])

    def add_block(block):
        cols = pl.ds(pl.multiple_of(block * feats, feats), feats)
        local_out[...] += nt(ho_all[block], out_w[:, cols])

    for k in range(1, line):
        hg.step(k)
        hg.other(k - 1, add_block)
        hg.column(k, add_block)
    hg.other(line - 1, add_block)
    gates = mod_all[:, mine][4:5]
    out_ref[...] = short(x_all[0:rows, mine].astype(jnp.float32) + gates * local_out[...])
    for copy in started:
        copy.wait_send()
    xg.drain()
    hg.drain()


def one_kernel(
    latent,
    context,
    conditioning,
    context_prompt_vector,
    shift_matrix,
    scale_matrix,
    residual_gate_matrix,
    query_matrix,
    key_matrix,
    value_matrix,
    gate_matrix,
    decay_down_factor,
    decay_up_factor,
    decay_key_bias,
    spike_log_decay,
    output_gain,
    output_matrix,
):
    n, s = lax.axis_size("tp"), lax.axis_size("sp")
    rows, feats = latent.shape
    crows = context.shape[0]
    heads = HEADS // n
    hk, hv = query_matrix.shape[0], value_matrix.shape[0]
    dv = hv // heads
    model = n * feats
    both = rows + crows
    inputs = conditioning.shape[0]
    bf, f32 = jnp.bfloat16, jnp.float32
    vmem, dma = pltpu.VMEM, pltpu.SemaphoreType.DMA
    pair = lambda k: [dma((k,)), dma((k,))]
    scratch = [
        vmem((both, model), bf),
        vmem((both, feats), bf),
        vmem((both, 2 * hk + 2 * hv), f32),
        vmem((both, 2 * DECAY_RANK), f32),
        vmem((3, feats, inputs), bf),
        vmem((2 * hk + 2 * hv, model), bf),
        vmem((output_matrix.shape[0], model), bf),
        vmem((2 * DECAY_RANK, model), bf),
        vmem((2, DECAY_RANK, hk), bf),
        vmem((2, hk), f32),
        vmem((2, HEADS, rows), f32),
        vmem((1, hv), f32),
        vmem((2, inputs // 128, 128), bf),
        vmem((8, feats), f32),
        vmem((s - 1, 8, feats), f32),
        vmem((8, model), f32),
        vmem((both, 2 * hk + 2 * hv), bf),
        vmem((s * crows, hk + hv), bf),
        vmem((s * crows, 128), f32),
        vmem((8, hk), f32),
        vmem((s - 1, 8, hk), f32),
        vmem((2, hk, dv), bf),
        vmem((s - 1, hk, dv), bf),
        vmem((rows, hv), f32),
        vmem((n, rows, hv), bf),
        dma((17,)),
    ]
    inner = 2 if n % 2 == 0 else 1
    line = n // inner
    hops = max(line - 1, 1)
    lanes = [dma((k, 2)) for k in (hops, hops, hops, hops, 2 * line - 1, 2 * line - 1)]
    scratch += lanes
    for count in (s - 1, n - 1, s - 1, s - 1, s - 1, s - 1):
        scratch += pair(count)
    scratch += lanes
    return pl.pallas_call(
        functools.partial(layer_kernel, n, s, inner, rows, crows, feats, heads, dv),
        out_shape=jax.ShapeDtypeStruct((rows, feats), bf),
        in_specs=[pl.BlockSpec(memory_space=pl.ANY)] * 17,
        out_specs=pl.BlockSpec(memory_space=pltpu.VMEM),
        scratch_shapes=scratch,
        compiler_params=pltpu.CompilerParams(
            collective_id=0, has_side_effects=True, vmem_limit_bytes=60 * 1024 * 1024
        ),
        name="layer",
    )(
        latent,
        context,
        conditioning.reshape(-1, 128),
        context_prompt_vector.reshape(-1, 128),
        shift_matrix,
        scale_matrix,
        residual_gate_matrix,
        query_matrix,
        key_matrix,
        value_matrix,
        gate_matrix,
        jnp.swapaxes(decay_down_factor, 1, 2).reshape(2 * DECAY_RANK, model),
        decay_up_factor,
        decay_key_bias,
        jnp.swapaxes(spike_log_decay, 1, 2),
        output_gain.reshape(1, -1),
        output_matrix,
    )


def solution(mesh):
    placed = (
        P("sp", "tp"),
        P("sp", "tp"),
        P("sp"),
        P("sp"),
        P("tp", "sp"),
        P("tp", "sp"),
        P("tp", "sp"),
        P("tp", None),
        P("tp", None),
        P("tp", None),
        P("tp", None),
        P(),
        P(),
        P(),
        P(None, "sp", None),
        P("tp"),
        P("tp", None),
    )
    whole_heads = HEADS % mesh.shape["tp"] == 0
    return jax.shard_map(
        one_kernel if whole_heads else local, mesh=mesh, in_specs=placed, out_specs=P("sp", "tp"), check_vma=False
    )
```

```python
import functools
import math

import jax
import jax.numpy as jnp
from jax import lax
from jax.experimental import pallas as pl
from jax.experimental.pallas import tpu as pltpu
from jax.sharding import PartitionSpec as P

D = 4096
HEADS = 16
DK = 128
DECAY_RANK = 16
BLK = 64
VGROUP = 64
MESH = pl.DeviceIdType.MESH


epsilon = 1e-05
gate_norm = 16.0
precise = lax.Precision.HIGHEST


def for_sending(value):

    def short(part):
        return part.astype(jnp.bfloat16) if part.dtype == jnp.float32 else part

    return jax.tree.map(short, value)


def from_partner(value, axis, distance):
    return lax.ppermute(value, axis, [(i, i ^ 1 << distance) for i in range(lax.axis_size(axis))])


def carried_in(value, axis, combine, identity, reverse):
    peers, index = (lax.axis_size(axis), lax.axis_index(axis))
    everything = jax.tree.map(
        lambda part, kind: lax.all_gather(part.astype(kind), axis),
        value,
        (jnp.bfloat16, jnp.bfloat16),
    )
    start = jax.tree.map(
        lambda part, zero: jnp.broadcast_to(jnp.asarray(zero, part.dtype), part.shape),
        value,
        identity,
    )

    def turn(k, before):
        at = peers - 1 - k if reverse else k
        reached = at > index if reverse else at < index
        new = combine(
            before, jax.tree.map(lambda part, own: part[at].astype(own.dtype), everything, value)
        )
        return jax.tree.map(lambda a, b: jnp.where(reached, a, b), new, before)

    return lax.fori_loop(0, peers, turn, start)


def linear(rows, weight):
    return lax.dot_general(
        rows, weight, (((1,), (1,)), ((), ())), preferred_element_type=jnp.float32
    )


def modulated(rows, row_sum, row_squares, shift_vec, scale_vec):
    rows_f = rows.astype(jnp.float32)
    mean_val = row_sum / D
    variance = row_squares / D - mean_val * mean_val
    return (
        (rows_f - mean_val) * lax.rsqrt(variance + epsilon) * (1.0 + scale_vec) + shift_vec
    ).astype(jnp.bfloat16)


def reverse_rows(array):
    return jnp.flip(array, axis=0)


def end_state(key_rows, value_rows, log_decay):
    cumulative = jnp.cumsum(log_decay, axis=0)
    totals = cumulative[-1]
    weighted = key_rows * jnp.exp(totals - cumulative)
    return (jnp.exp(totals), jnp.einsum("nhd,nhe->hde", weighted, value_rows, precision=precise))


def combine(earlier, later):
    return (earlier[0] * later[0], later[0][..., None] * earlier[1] + later[1])


def blockwise(queries, key_rows, value_rows, log_decay, carried, block_len):
    length, head_count, _ = queries.shape
    value_width = value_rows.shape[-1]
    blocks = length // block_len

    def shaped(array):
        return array.reshape(blocks, block_len, head_count, array.shape[-1])

    triangle = jnp.tril(jnp.ones((block_len, block_len), jnp.float32))

    def advance(state_now, inputs):
        block_q, block_k, block_v, block_a = inputs
        cumulative = jnp.cumsum(block_a, axis=0)
        block_end = cumulative[-1]
        query_dec = block_q * jnp.exp(cumulative)
        scores = (
            jnp.einsum("ihd,jhd->hij", query_dec, block_k * jnp.exp(-cumulative), precision=precise)
            * triangle
        )
        result = jnp.einsum("hij,jhe->ihe", scores, block_v, precision=precise)
        result = result + jnp.einsum("ihd,hde->ihe", query_dec, state_now, precision=precise)
        state_next = state_now * jnp.exp(block_end)[:, :, None] + jnp.einsum(
            "jhd,jhe->hde", block_k * jnp.exp(block_end - cumulative), block_v, precision=precise
        )
        return (state_next, result)

    _, outputs = lax.scan(
        advance, carried, (shaped(queries), shaped(key_rows), shaped(value_rows), shaped(log_decay))
    )
    return outputs.reshape(length, head_count, value_width)


def head_channels(pieces, per_head, tp_index):
    for bit_number in range(per_head.bit_length() - 1):
        partner = from_partner(
            (for_sending(pieces[0]), for_sending(pieces[1]), for_sending(pieces[2])),
            "tp",
            bit_number,
        )
        upper = tp_index // (1 << bit_number) % 2 == 1
        pieces = tuple(
            (
                jnp.where(
                    upper,
                    jnp.concatenate([theirs, mine], axis=1),
                    jnp.concatenate([mine, theirs], axis=1),
                )
                for mine, theirs in zip(pieces, partner)
            )
        )
    return pieces


def context_totals(fwd_growth, fwd_state, bwd_growth, bwd_state, identity):

    def absorb(carried, piece):
        return (combine(carried, piece), None)

    total_fwd, _ = lax.scan(absorb, identity, (fwd_growth, fwd_state))
    total_bwd, _ = lax.scan(absorb, identity, (bwd_growth, bwd_state), reverse=True)
    return (total_fwd, total_bwd)


def stored(array):
    return lax.optimization_barrier(array.astype(jnp.bfloat16))


def local(
    latent,
    context,
    conditioning,
    context_prompt_vector,
    shift_matrix,
    scale_matrix,
    residual_gate_matrix,
    query_matrix,
    key_matrix,
    value_matrix,
    gate_matrix,
    decay_down_factor,
    decay_up_factor,
    decay_key_bias,
    spike_log_decay,
    output_gain,
    output_matrix,
):
    tp_count = lax.axis_size("tp")
    tp_index = lax.axis_index("tp")
    per_head = max(tp_count // HEADS, 1)
    heads_per_shard = max(HEADS // tp_count, 1)
    leading_head = tp_index // per_head * heads_per_shard
    tok_rows = latent.shape[0]
    conds = jax.nn.silu(
        jnp.stack([conditioning, context_prompt_vector]).astype(jnp.float32)
    ).astype(jnp.bfloat16)
    shifts, scales, gates = lax.psum(
        (
            linear(conds, shift_matrix),
            linear(conds, scale_matrix),
            linear(conds, residual_gate_matrix),
        ),
        "sp",
    )
    down_both = jnp.concatenate([decay_down_factor[0].T, decay_down_factor[1].T], axis=0)
    lat_weights = (query_matrix, key_matrix, value_matrix, gate_matrix, down_both)
    ctx_weights = (key_matrix, value_matrix, down_both)
    lat_f = latent.astype(jnp.float32)
    ctx_f = context.astype(jnp.float32)
    lat_sum, lat_squares, ctx_sum, ctx_squares = lax.psum(
        (
            jnp.sum(lat_f, axis=1, keepdims=True),
            jnp.sum(lat_f * lat_f, axis=1, keepdims=True),
            jnp.sum(ctx_f, axis=1, keepdims=True),
            jnp.sum(ctx_f * ctx_f, axis=1, keepdims=True),
        ),
        "tp",
    )
    latent_normalized = modulated(latent, lat_sum, lat_squares, shifts[0], scales[0])
    normed_ctx = modulated(context, ctx_sum, ctx_squares, shifts[1], scales[1])
    lat_piece = lax.all_gather(latent_normalized, "tp", axis=1, tiled=True)
    ctx_piece = lax.all_gather(normed_ctx, "tp", axis=1, tiled=True)
    lat_new = tuple((linear(lat_piece, weight) for weight in lat_weights))
    ctx_new = tuple((linear(ctx_piece, weight) for weight in ctx_weights))
    query_part, key_part, value_part, gate_part, low_rank_part = lat_new
    ctx_key_part, ctx_value_part, ctx_low = ctx_new
    query_full, key_full, ctx_key_full = head_channels(
        (stored(query_part), stored(key_part), stored(ctx_key_part)), per_head, tp_index
    )

    def split_heads(rows, width):
        return rows.astype(jnp.float32).reshape(rows.shape[0], heads_per_shard, width)

    value_cols = value_part.shape[1] // heads_per_shard
    queries = split_heads(query_full, DK) * DK ** (-0.5)
    key_rows = split_heads(key_full, DK)
    ctx_keys = split_heads(ctx_key_full, DK)
    values_lat = split_heads(stored(value_part), value_cols)
    values_ctx = split_heads(stored(ctx_value_part), value_cols)
    gate_rows = stored(gate_part).astype(jnp.float32)

    def per_head_decay(low_rows, direction):
        up_part = lax.dynamic_slice_in_dim(
            decay_up_factor[direction], leading_head * DK, heads_per_shard * DK, 1
        ).astype(jnp.float32)
        bias_part = lax.dynamic_slice_in_dim(
            decay_key_bias[direction], leading_head * DK, heads_per_shard * DK, 0
        )
        pre_act = jnp.dot(low_rows, up_part, precision=precise) + bias_part
        return (jax.nn.log_sigmoid(pre_act) / gate_norm).reshape(
            low_rows.shape[0], heads_per_shard, DK
        )

    decay_spikes = lax.dynamic_slice_in_dim(spike_log_decay, leading_head, heads_per_shard, 2)
    latent_forward = per_head_decay(low_rank_part[:, :DECAY_RANK], 0) + decay_spikes[0][:, :, None]
    latent_backward = per_head_decay(low_rank_part[:, DECAY_RANK:], 1) + decay_spikes[1][:, :, None]
    ctx_fwd = per_head_decay(ctx_low[:, :DECAY_RANK], 0)
    ctx_bwd = per_head_decay(ctx_low[:, DECAY_RANK:], 1)
    cf_growth, cf_state = end_state(ctx_keys, values_ctx, ctx_fwd)
    cb_growth, cb_state = end_state(
        reverse_rows(ctx_keys), reverse_rows(values_ctx), reverse_rows(ctx_bwd)
    )
    lf_growth, lf_state = end_state(key_rows, values_lat, latent_forward)
    lb_growth, lb_state = end_state(
        reverse_rows(key_rows), reverse_rows(values_lat), reverse_rows(latent_backward)
    )
    identity = (
        jnp.ones((heads_per_shard, DK), jnp.float32),
        jnp.zeros((heads_per_shard, DK, value_cols), jnp.float32),
    )
    ctx_gathered = (
        lax.all_gather(cf_growth[None].astype(jnp.bfloat16), "sp", axis=0, tiled=True).astype(
            jnp.float32
        ),
        lax.all_gather(cf_state[None].astype(jnp.bfloat16), "sp", axis=0, tiled=True).astype(
            jnp.float32
        ),
        lax.all_gather(cb_growth[None].astype(jnp.bfloat16), "sp", axis=0, tiled=True).astype(
            jnp.float32
        ),
        lax.all_gather(cb_state[None].astype(jnp.bfloat16), "sp", axis=0, tiled=True).astype(
            jnp.float32
        ),
    )
    total_fwd, total_bwd = context_totals(
        ctx_gathered[0], ctx_gathered[1], ctx_gathered[2], ctx_gathered[3], identity
    )
    prefix = carried_in((lf_growth, lf_state), "sp", combine, identity, False)
    suffix = carried_in((lb_growth, lb_state), "sp", combine, identity, True)
    start_fwd = combine(total_fwd, prefix)[1]
    start_bwd = combine(total_bwd, suffix)[1]
    zero_state = jnp.zeros((heads_per_shard, DK, value_cols), jnp.float32)

    def direction_out(query_rows, key_list, value_list, log_decay, start_state):
        local_part = blockwise(query_rows, key_list, value_list, log_decay, zero_state, BLK)
        reach = query_rows * jnp.exp(jnp.cumsum(log_decay, axis=0))
        return local_part + jnp.einsum("nhd,hde->nhe", reach, start_state, precision=precise)

    out_fwd = direction_out(queries, key_rows, values_lat, latent_forward, start_fwd)
    out_bwd = reverse_rows(
        direction_out(
            reverse_rows(queries),
            reverse_rows(key_rows),
            reverse_rows(values_lat),
            reverse_rows(latent_backward),
            start_bwd,
        )
    )
    grouped = (out_fwd + out_bwd).reshape(tok_rows, -1, VGROUP)
    grouped = grouped * lax.rsqrt(jnp.mean(grouped * grouped, axis=-1, keepdims=True) + epsilon)
    heads_out = (grouped.reshape(tok_rows, -1) * output_gain * jax.nn.silu(gate_rows)).astype(
        jnp.bfloat16
    )
    branch = linear(lax.all_gather(heads_out, "tp", axis=1, tiled=True), output_matrix)
    return (latent.astype(jnp.float32) + gates[0] * branch).astype(jnp.bfloat16)


def exact(a, b):
    return lax.dot_general(
        a, b, (((1,), (0,)), ((), ())), precision=precise, preferred_element_type=jnp.float32
    )


def nt(a, b):
    return lax.dot_general(a, b, (((1,), (1,)), ((), ())), preferred_element_type=jnp.float32)


def nn(a, b):
    return lax.dot_general(a, b, (((1,), (0,)), ((), ())), preferred_element_type=jnp.float32)


def tn(a, b):
    return lax.dot_general(a, b, (((0,), (0,)), ((), ())), preferred_element_type=jnp.float32)


def short(value):
    return value.astype(jnp.bfloat16)


def log_decay_of(low, up, bias):
    pre = exact(low, up) + bias
    return (jnp.minimum(pre, 0.0) - jnp.log1p(jnp.exp(-jnp.abs(pre)))) / gate_norm


def triangle_of(size, upper):
    i = lax.broadcasted_iota(jnp.int32, (size, size), 0)
    j = lax.broadcasted_iota(jnp.int32, (size, size), 1)
    return (j >= i) if upper else (j <= i)


def layer_kernel(
    n,
    s,
    inner,
    rows,
    crows,
    feats,
    heads,
    dv,
    latent,
    context,
    conditioning,
    prompt,
    shift_m,
    scale_m,
    gate_m,
    query_m,
    key_m,
    value_m,
    og_m,
    down,
    up,
    bias,
    spike,
    gain,
    out_m,
    out_ref,
    x_all,
    xn,
    acc,
    low_acc,
    mod_w,
    proj_w,
    out_w,
    down_v,
    up_v,
    bias_v,
    spike_v,
    gain_v,
    cond_v,
    mod_own,
    mod_recv,
    mod_all,
    proj,
    ctx_kv,
    ctx_low,
    tot_own,
    tot_recv,
    st_own,
    st_recv,
    local_out,
    ho_all,
    load_sem,
    xs_up,
    xr_up,
    xs_dn,
    xr_dn,
    xs_y,
    xr_y,
    m1_s,
    m1_r,
    m2_s,
    m2_r,
    kv_s,
    kv_r,
    lo_s,
    lo_r,
    to_s,
    to_r,
    st_s,
    st_r,
    hs_up,
    hr_up,
    hs_dn,
    hr_dn,
    hs_y,
    hr_y,
):
    me = lax.axis_index("tp")
    sp = lax.axis_index("sp")
    hk = heads * DK
    hv = heads * dv
    model = n * feats
    mine = pl.ds(pl.multiple_of(me * feats, feats), feats)

    loads = []

    def load(src, dst):
        copy = pltpu.make_async_copy(src, dst, load_sem.at[len(loads)])
        loads.append(copy)
        copy.start()
        return copy

    first = [
        load(conditioning, cond_v.at[0]),
        load(prompt, cond_v.at[1]),
        load(shift_m, mod_w.at[0]),
        load(scale_m, mod_w.at[1]),
        load(gate_m, mod_w.at[2]),
    ]
    own_x = [
        load(latent, x_all.at[pl.ds(0, rows), mine]),
        load(context, x_all.at[pl.ds(rows, crows), mine]),
    ]
    weights = [
        load(query_m, proj_w.at[pl.ds(0, hk)]),
        load(key_m, proj_w.at[pl.ds(hk, hk)]),
        load(value_m, proj_w.at[pl.ds(2 * hk, hv)]),
        load(og_m, proj_w.at[pl.ds(2 * hk + hv, hv)]),
        load(down, down_v),
    ]
    head_cols = pl.ds(pl.multiple_of(me * hk, hk), hk)
    small = [
        load(up.at[:, :, head_cols], up_v),
        load(bias.at[:, head_cols], bias_v),
        load(spike, spike_v),
        load(gain, gain_v),
    ]
    last = load(out_m, out_w)

    barrier = pltpu.get_barrier_semaphore()
    for d in range(1, n):
        pl.semaphore_signal(
            barrier, inc=1, device_id={"tp": lax.rem(me + d, n)}, device_id_type=MESH
        )
    for d in range(1, s):
        pl.semaphore_signal(
            barrier, inc=1, device_id={"sp": lax.rem(sp + d, s)}, device_id_type=MESH
        )
    pl.semaphore_wait(barrier, n - 1 + s - 1)

    started = []

    def send(src, dst, send_sem, recv_sem, axis, d):
        index, count = (me, n) if axis == "tp" else (sp, s)
        copy = pltpu.make_async_remote_copy(
            src_ref=src,
            dst_ref=dst,
            send_sem=send_sem.at[d - 1],
            recv_sem=recv_sem.at[d - 1],
            device_id={axis: lax.rem(index + d, count)},
            device_id_type=MESH,
        )
        copy.start()
        started.append(copy)
        return copy

    line = n // inner
    z, y = lax.div(me, inner), lax.rem(me, inner)

    def block_of(at, column):
        return at * inner + column

    class Gather:
        def __init__(self, view, pieces, up, down, across):
            self.view, self.pieces = view, pieces
            self.lanes = {"up": up, "down": down, "across": across}

        def copy(self, lane, block, piece, slot, target):
            sends, recvs = self.lanes[lane]
            ref = self.view(block, piece)
            return pltpu.make_async_remote_copy(
                src_ref=ref,
                dst_ref=ref,
                send_sem=sends.at[slot, piece],
                recv_sem=recvs.at[slot, piece],
                device_id={"tp": target},
                device_id_type=MESH,
            )

        def hop(self, lane, at, piece, slot):
            target = {
                "up": block_of(jnp.minimum(z + 1, line - 1), y),
                "down": block_of(jnp.maximum(z - 1, 0), y),
                "across": block_of(z, inner - 1 - y),
            }[lane]
            return self.copy(lane, block_of(at, y), piece, slot, target)

        def sends(self, k, piece, act):
            for lane, at, has, onward, slot in (
                ("up", z - k, z >= k, z + 1 < line, max(2 * k - 1, 0)),
                ("down", z + k, z + k < line, z > 0, 2 * k),
            ):
                if k < line - 1:
                    pl.when(has & onward)(lambda: act(self.hop(lane, at, piece, k)))
                if inner > 1 and (k > 0 or lane == "up"):
                    pl.when(has)(lambda: act(self.hop("across", at, piece, slot)))

        def start(self):
            for piece in range(self.pieces):
                self.sends(0, piece, lambda c: c.start())

        def step(self, k):
            for piece in range(self.pieces):
                for lane, at, has in (("up", z - k, z >= k), ("down", z + k, z + k < line)):
                    pl.when(has)(lambda: self.hop(lane, at, piece, k - 1).wait_recv())
                self.sends(k, piece, lambda c: c.start())

        def column(self, k, work):
            pl.when(z >= k)(lambda: work(block_of(z - k, y)))
            pl.when(z + k < line)(lambda: work(block_of(z + k, y)))

        def other(self, k, work):
            if inner == 1:
                return

            def arrive(at, slot):
                block = block_of(at, inner - 1 - y)
                for piece in range(self.pieces):
                    self.copy("across", block, piece, slot, block).wait_recv()
                work(block)

            if k == 0:
                arrive(z, 0)
                return
            pl.when(z >= k)(lambda: arrive(z - k, 2 * k - 1))
            pl.when(z + k < line)(lambda: arrive(z + k, 2 * k))

        def drain(self):
            for k in range(line):
                for piece in range(self.pieces):
                    self.sends(k, piece, lambda c: c.wait_send())

    both = rows + crows
    cut = both // 32 * 16

    def x_view(block, piece):
        part = pl.ds(0, cut) if piece == 0 else pl.ds(cut, both - cut)
        return x_all.at[part, pl.ds(pl.multiple_of(block * feats, feats), feats)]

    xg = Gather(x_view, 2, (xs_up, xr_up), (xs_dn, xr_dn), (xs_y, xr_y))
    for copy in own_x:
        copy.wait()
    xg.start()

    for copy in first:
        copy.wait()
    def one_row(which):
        part = cond_v[which].astype(jnp.float32)
        return jnp.concatenate([part[r : r + 1] for r in range(part.shape[0])], axis=1)

    row_of = lax.broadcasted_iota(jnp.int32, (16, shift_m.shape[1]), 0)
    conds = jnp.where(row_of == 0, one_row(0), one_row(1))
    conds = short(conds * lax.logistic(conds))
    for which in range(3):
        mod_own[2 * which : 2 * which + 2, :] = nt(conds, mod_w[which])[0:2]
    mod_own[6:8, :] = jnp.zeros((2, feats), jnp.float32)
    m1 = {
        d: send(mod_own, mod_recv.at[d - 1], m1_s, m1_r, "sp", d) for d in range(1, s)
    }

    own = x_all[:, mine]
    ones = jnp.ones((16, feats), jnp.bfloat16)
    own_f = own.astype(jnp.float32)
    rest = own_f * own_f
    row_squares = jnp.zeros((16, both), jnp.float32)
    for _ in range(3):
        top = short(rest)
        row_squares = row_squares + nt(ones, top)
        rest = rest - top.astype(jnp.float32)
    row_sum = nt(ones, own)

    if line > 1:
        xg.step(1)
    for d in range(1, s):
        m1[d].wait_recv()
    total = mod_own[...]
    for d in range(1, s):
        total = total + mod_recv[d - 1]
    mod_all[:, mine] = total
    stat_cols = pl.ds(pl.multiple_of(me * feats, feats), both)
    mod_all[6:7, stat_cols] = row_sum[0:1]
    mod_all[7:8, stat_cols] = row_squares[0:1]
    m2 = {
        d: send(mod_all.at[:, mine], mod_all.at[:, mine], m2_s, m2_r, "tp", d)
        for d in range(1, n)
    }
    tile = math.gcd(2 * hk + 2 * hv, 512)
    columns = acc.shape[1]
    acc[...] = jnp.zeros(acc.shape, jnp.float32)
    low_acc[...] = jnp.zeros(low_acc.shape, jnp.float32)

    def moments():
        for d in range(1, n):
            m2[d].wait_recv()
        diagonal = lax.broadcasted_iota(jnp.int32, (both, both), 0) == lax.broadcasted_iota(
            jnp.int32, (both, both), 1
        )

        def column_of(row):
            whole_row = sum(mod_all[row : row + 1, b * feats : b * feats + both] for b in range(n))
            return jnp.sum(jnp.where(diagonal, whole_row, 0.0), axis=1, keepdims=True) / model

        mean = column_of(6)
        return mean, lax.rsqrt(column_of(7) - mean * mean + epsilon)

    def project_block(block, mean, spread):
        cols = pl.ds(pl.multiple_of(block * feats, feats), feats)
        x = (x_all[:, cols].astype(jnp.float32) - mean) * spread
        mod = mod_all[:, cols]
        xn[0:rows, :] = short(x[0:rows] * (1.0 + mod[2:3]) + mod[0:1])
        xn[rows:, :] = short(x[rows:] * (1.0 + mod[3:4]) + mod[1:2])
        low_acc[...] += nt(xn[...], down_v[:, cols])

        for t in range(columns // tile):
            out = slice(t * tile, (t + 1) * tile)
            acc[:, out] += nt(xn[...], proj_w[out, cols])

    ready = None
    for k in range(2, line + 1):
        if k < line:
            xg.step(k)
        if ready is None:
            ready = moments()
            for copy in weights:
                copy.wait()
            work = lambda block: project_block(block, *ready)
            work(me)
        xg.column(k - 1, work)
        xg.other(k - 2, work)
    xg.other(line - 1, work)
    proj[...] = short(acc[...])

    own_ctx = pl.ds(pl.multiple_of(sp * crows, crows), crows)
    ctx_kv[own_ctx, :] = proj[rows:, hk : 2 * hk + hv]
    ctx_low[own_ctx, :] = jnp.zeros((crows, ctx_low.shape[1]), jnp.float32)
    ctx_low[own_ctx, 0 : 2 * DECAY_RANK] = low_acc[rows:]
    kv = {
        d: send(ctx_kv.at[own_ctx], ctx_kv.at[own_ctx], kv_s, kv_r, "sp", d)
        for d in range(1, s)
    }
    lo = {
        d: send(ctx_low.at[own_ctx], ctx_low.at[own_ctx], lo_s, lo_r, "sp", d)
        for d in range(1, s)
    }

    for copy in small:
        copy.wait()
    slot_head = lax.broadcasted_iota(jnp.int32, (spike_v.shape[1], hk), 0)
    lane_head = lax.broadcasted_iota(jnp.int32, (spike_v.shape[1], hk), 1) // DK
    pick = jnp.where(slot_head == me * heads + lane_head, 1.0, 0.0)
    none = jnp.zeros((DECAY_RANK, hk), jnp.float32)
    ups = [
        jnp.concatenate([up_v[0].astype(jnp.float32), none], axis=0),
        jnp.concatenate([none, up_v[1].astype(jnp.float32)], axis=0),
    ]
    cum = []
    for direction in range(2):
        logs = log_decay_of(low_acc[0:rows], ups[direction], bias_v[direction : direction + 1])
        logs = logs + lax.dot_general(
            spike_v[direction],
            pick,
            (((0,), (0,)), ((), ())),
            precision=precise,
            preferred_element_type=jnp.float32,
        )
        cum.append(exact(triangle_of(rows, direction == 1).astype(jnp.float32), logs))
    whole = [cum[0][rows - 1 : rows], cum[1][0:1]]
    tot_own[0:1, :] = whole[0]
    tot_own[1:2, :] = whole[1]
    tot_own[2:8, :] = jnp.zeros((6, hk), jnp.float32)
    to = {d: send(tot_own, tot_recv.at[d - 1], to_s, to_r, "sp", d) for d in range(1, s)}

    keys = proj[0:rows, hk : 2 * hk].astype(jnp.float32)
    for direction in range(2):
        weighted = short(keys * jnp.exp(whole[direction] - cum[direction]))
        for h in range(heads):
            st_own[direction, h * DK : (h + 1) * DK, :] = short(
                tn(
                    weighted[:, h * DK : (h + 1) * DK],
                    proj[0:rows, 2 * hk + h * dv : 2 * hk + (h + 1) * dv],
                )
            )
    st = {}
    for d in range(1, s):
        later = lax.rem(sp + d, s) > sp
        st[d] = send(
            st_own.at[jnp.where(later, 0, 1)], st_recv.at[d - 1], st_s, st_r, "sp", d
        )

    queries = proj[0:rows, 0:hk].astype(jnp.float32) * DK ** (-0.5)
    blocks = rows // BLK

    def span(b):
        return slice(b * BLK, (b + 1) * BLK)

    inside = [[], []]
    for b in range(blocks):
        f = cum[0][span(b)]
        inside[0].append(f if b == 0 else f - cum[0][b * BLK - 1 : b * BLK])
        f = cum[1][span(b)]
        inside[1].append(
            f if b == blocks - 1 else f - cum[1][(b + 1) * BLK : (b + 1) * BLK + 1]
        )
    ends = [[part[BLK - 1 : BLK] for part in inside[0]], [part[0:1] for part in inside[1]]]
    q_dec = [[short(queries[span(b)] * jnp.exp(inside[e][b])) for b in range(blocks)] for e in range(2)]
    k_dec = [[short(keys[span(b)] * jnp.exp(-inside[e][b])) for b in range(blocks)] for e in range(2)]
    k_end = [
        [short(keys[span(b)] * jnp.exp(ends[e][b] - inside[e][b])) for b in range(blocks)]
        for e in range(2)
    ]
    lower, upper = triangle_of(BLK, False), triangle_of(BLK, True)
    for h in range(heads):
        ch = slice(h * DK, (h + 1) * DK)
        lines = []
        for b in range(blocks):
            strip = []
            for c in range(blocks):
                if b == c:
                    strip.append(
                        jnp.where(lower, nt(q_dec[0][b][:, ch], k_dec[0][b][:, ch]), 0.0)
                        + jnp.where(upper, nt(q_dec[1][b][:, ch], k_dec[1][b][:, ch]), 0.0)
                    )
                    continue
                e = 0 if c < b else 1
                near = q_dec[e][b][:, ch]
                between = range(c + 1, b) if c < b else range(b + 1, c)
                if len(between) > 0:
                    gap = sum(ends[e][m][:, ch] for m in between)
                    near = short(queries[span(b)][:, ch] * jnp.exp(inside[e][b][:, ch] + gap))
                strip.append(nt(near, k_end[e][c][:, ch]))
            lines.append(jnp.concatenate(strip, axis=1) if blocks > 1 else strip[0])
        scores = short(jnp.concatenate(lines, axis=0) if blocks > 1 else lines[0])
        local_out[:, h * dv : (h + 1) * dv] = nn(
            scores, proj[0:rows, 2 * hk + h * dv : 2 * hk + (h + 1) * dv]
        )

    for d in range(1, s):
        kv[d].wait_recv()
        lo[d].wait_recv()
    ctx_keys = ctx_kv[:, 0:hk].astype(jnp.float32)
    ctx_states = []
    for direction in range(2):
        logs = log_decay_of(
            ctx_low[:, 0 : 2 * DECAY_RANK],
            ups[direction],
            bias_v[direction : direction + 1],
        )
        length = s * crows
        c = exact(triangle_of(length, direction == 1).astype(jnp.float32), logs)
        end = c[length - 1 : length] if direction == 0 else c[0:1]
        weighted = short(ctx_keys * jnp.exp(end - c))
        ctx_states.append(
            [
                short(
                    tn(
                        weighted[:, h * DK : (h + 1) * DK],
                        ctx_kv[:, hk + h * dv : hk + (h + 1) * dv],
                    )
                )
                for h in range(heads)
            ]
        )

    for d in range(1, s):
        to[d].wait_recv()
    places = {d: lax.rem(sp - d + s, s) for d in range(1, s)}

    def passed(low_end, high_end, direction):
        result = jnp.zeros((1, hk), jnp.float32)
        for d in range(1, s):
            held = jnp.where((places[d] > low_end) & (places[d] < high_end), 1.0, 0.0)
            result = result + held * tot_recv[d - 1][direction : direction + 1]
        return result

    ctx_reach = [
        short(queries * jnp.exp(cum[0] + passed(-1, sp, 0))),
        short(queries * jnp.exp(cum[1] + passed(sp, s, 1))),
    ]
    for h in range(heads):
        ch = slice(h * DK, (h + 1) * DK)
        local_out[:, h * dv : (h + 1) * dv] += nn(
            jnp.concatenate([r[:, ch] for r in ctx_reach], axis=1),
            jnp.concatenate([ctx_states[e][h] for e in range(2)], axis=0),
        )
    reach = []
    for d in range(1, s):
        p = places[d]
        before = jnp.where(p < sp, 1.0, 0.0)
        exponent = before * (cum[0] + passed(p, sp, 0)) + (1.0 - before) * (
            cum[1] + passed(sp, p, 1)
        )
        reach.append(short(queries * jnp.exp(exponent)))
    gate_rows = proj[0:rows, 2 * hk + hv :].astype(jnp.float32)
    small_gate = gate_rows * lax.logistic(gate_rows) * gain_v[...]
    gi = lax.broadcasted_iota(jnp.int32, (dv, dv), 0) // VGROUP
    gj = lax.broadcasted_iota(jnp.int32, (dv, dv), 1) // VGROUP
    group = jnp.where(gi == gj, 1.0, 0.0).astype(jnp.bfloat16)
    for d in range(1, s):
        st[d].wait_recv()
    for h in range(heads):
        ch = slice(h * DK, (h + 1) * DK)
        vc = slice(h * dv, (h + 1) * dv)
        o = local_out[:, vc]
        for d in range(1, s):
            o = o + nn(reach[d - 1][:, ch], st_recv[d - 1, ch, :])
        squares = o * o
        top = short(squares)
        rest = short(squares - top.astype(jnp.float32))
        power = (nn(top, group) + nn(rest, group)) * (1.0 / VGROUP)
        ho_all[me, :, vc] = short(o * lax.rsqrt(power + epsilon) * small_gate[:, vc])

    def ho_view(block, piece):
        return ho_all.at[block, pl.ds(piece * (rows // 4), rows // 4)]

    hg = Gather(ho_view, 4, (hs_up, hr_up), (hs_dn, hr_dn), (hs_y, hr_y))
    hg.start()
    last.wait()
    local_out[...] = nt(ho_all[me], out_w[:, mine])

    def add_block(block):
        cols = pl.ds(pl.multiple_of(block * feats, feats), feats)
        local_out[...] += nt(ho_all[block], out_w[:, cols])

    for k in range(1, line):
        hg.step(k)
        hg.other(k - 1, add_block)
        hg.column(k, add_block)
    hg.other(line - 1, add_block)
    gates = mod_all[:, mine][4:5]
    out_ref[...] = short(x_all[0:rows, mine].astype(jnp.float32) + gates * local_out[...])
    for copy in started:
        copy.wait_send()
    xg.drain()
    hg.drain()


def one_kernel(
    latent,
    context,
    conditioning,
    context_prompt_vector,
    shift_matrix,
    scale_matrix,
    residual_gate_matrix,
    query_matrix,
    key_matrix,
    value_matrix,
    gate_matrix,
    decay_down_factor,
    decay_up_factor,
    decay_key_bias,
    spike_log_decay,
    output_gain,
    output_matrix,
):
    n, s = lax.axis_size("tp"), lax.axis_size("sp")
    rows, feats = latent.shape
    crows = context.shape[0]
    heads = HEADS // n
    hk, hv = query_matrix.shape[0], value_matrix.shape[0]
    dv = hv // heads
    model = n * feats
    both = rows + crows
    inputs = conditioning.shape[0]
    bf, f32 = jnp.bfloat16, jnp.float32
    vmem, dma = pltpu.VMEM, pltpu.SemaphoreType.DMA
    pair = lambda k: [dma((k,)), dma((k,))]
    scratch = [
        vmem((both, model), bf),
        vmem((both, feats), bf),
        vmem((both, 2 * hk + 2 * hv), f32),
        vmem((both, 2 * DECAY_RANK), f32),
        vmem((3, feats, inputs), bf),
        vmem((2 * hk + 2 * hv, model), bf),
        vmem((output_matrix.shape[0], model), bf),
        vmem((2 * DECAY_RANK, model), bf),
        vmem((2, DECAY_RANK, hk), bf),
        vmem((2, hk), f32),
        vmem((2, HEADS, rows), f32),
        vmem((1, hv), f32),
        vmem((2, inputs // 128, 128), bf),
        vmem((8, feats), f32),
        vmem((s - 1, 8, feats), f32),
        vmem((8, model), f32),
        vmem((both, 2 * hk + 2 * hv), bf),
        vmem((s * crows, hk + hv), bf),
        vmem((s * crows, 128), f32),
        vmem((8, hk), f32),
        vmem((s - 1, 8, hk), f32),
        vmem((2, hk, dv), bf),
        vmem((s - 1, hk, dv), bf),
        vmem((rows, hv), f32),
        vmem((n, rows, hv), bf),
        dma((17,)),
    ]
    inner = 2 if n % 2 == 0 else 1
    line = n // inner
    hops = max(line - 1, 1)
    counts = (hops, hops, hops, hops, 2 * line - 1, 2 * line - 1)
    scratch += [dma((k, 2)) for k in counts]
    for count in (s - 1, n - 1, s - 1, s - 1, s - 1, s - 1):
        scratch += pair(count)
    scratch += [dma((k, 4)) for k in counts]
    return pl.pallas_call(
        functools.partial(layer_kernel, n, s, inner, rows, crows, feats, heads, dv),
        out_shape=jax.ShapeDtypeStruct((rows, feats), bf),
        in_specs=[pl.BlockSpec(memory_space=pl.ANY)] * 17,
        out_specs=pl.BlockSpec(memory_space=pltpu.VMEM),
        scratch_shapes=scratch,
        compiler_params=pltpu.CompilerParams(
            collective_id=0, has_side_effects=True, vmem_limit_bytes=60 * 1024 * 1024
        ),
        name="layer",
    )(
        latent,
        context,
        conditioning.reshape(-1, 128),
        context_prompt_vector.reshape(-1, 128),
        shift_matrix,
        scale_matrix,
        residual_gate_matrix,
        query_matrix,
        key_matrix,
        value_matrix,
        gate_matrix,
        jnp.swapaxes(decay_down_factor, 1, 2).reshape(2 * DECAY_RANK, model),
        decay_up_factor,
        decay_key_bias,
        jnp.swapaxes(spike_log_decay, 1, 2),
        output_gain.reshape(1, -1),
        output_matrix,
    )


def solution(mesh):
    placed = (
        P("sp", "tp"),
        P("sp", "tp"),
        P("sp"),
        P("sp"),
        P("tp", "sp"),
        P("tp", "sp"),
        P("tp", "sp"),
        P("tp", None),
        P("tp", None),
        P("tp", None),
        P("tp", None),
        P(),
        P(),
        P(),
        P(None, "sp", None),
        P("tp"),
        P("tp", None),
    )
    whole_heads = HEADS % mesh.shape["tp"] == 0
    return jax.shard_map(
        one_kernel if whole_heads else local, mesh=mesh, in_specs=placed, out_specs=P("sp", "tp"), check_vma=False
    )
```
